32 devices in a mesh: row: 16 (over z, y, x), col: 2 (over core).
Axes of the slice: x: 2, y: 2, z: 4, core: 2. Of those that a mesh axis runs over, the one named last changes fastest.
Arguments:
- tokens: bfloat16 [2, 3072, 2048], P('col', 'row'), may hold values from -6 to 6
- proj_in: bfloat16 [2048, 512], P('col'), may hold values from -0.125 to 0.125
- proj_out: bfloat16 [512, 2048], P(None, 'row'), may hold values from -0.25 to 0.25
Outputs:
- output: bfloat16 [2, 3072, 2048], P('col', 'row')
The draws below stay inside these ranges and needn't reach their ends.
All inputs are finite; a program needn't handle non-finite values.
Results may differ from the reference program's by a relative error of at most 0.0083.
Values may be sent and summed in bfloat16 or wider, within the bound.
No kernel may reach another device: no remote copies, remote signals or barrier semaphores. Data moves between devices by JAX's collectives and lax.ppermute only.
A program may use at most 64 MiB of HBM per device.

```python
import jax
import jax.numpy as jnp
from jax import lax

D = 2048
GROUPS = 4
GRP = 128
FW = 512
LEN = 3072
BATCH = 2


def steps_of(rng, extent, split, smallest, largest):
    level = 1.0
    for axis_at, shards_of in split:
        draws = jax.random.uniform(jax.random.fold_in(jax.random.fold_in(rng, 6), axis_at), (shards_of,), jnp.float32, smallest / len(split), largest / len(split))
        level = level * jnp.repeat(jnp.exp(draws), extent[axis_at] // shards_of).reshape((-1,) + (1,) * (len(extent) - 1 - axis_at))
    return level


def scatter_about(own_key, shape, spread, reach, pieces=(), kind=jnp.bfloat16):
    gain = steps_of(own_key, shape, pieces, -0.22, 0.18) if pieces else 1.0
    values = jax.random.normal(own_key, shape, jnp.float32) * spread * gain
    return jnp.minimum(jnp.maximum(values, -reach), reach).astype(kind)


def setup_inputs(seed: int = 0) -> dict:
    seeds = jax.random.split(jax.random.key(seed), 4)
    return {
        "tokens": scatter_about(seeds[0], (BATCH, LEN, D), 1.0, 6.0, ((0, 2), (1, 16))),
        "proj_in": scatter_about(seeds[1], (D, FW), D ** -0.5, 0.125, ((0, 2),)),
        "proj_out": scatter_about(seeds[2], (FW, D), FW ** -0.5, 0.25, ((1, 16),)),
    }


def reference(tokens, proj_in, proj_out):
    def one_sequence(seq):
        mapped = jnp.dot(seq, proj_in, preferred_element_type=jnp.float32).astype(jnp.bfloat16)
        length = seq.shape[0]
        grid = mapped.astype(jnp.float32).reshape(length, GROUPS, GRP)
        spectrum = jnp.fft.fft2(grid, axes=(0, 2), norm="ortho").real
        mixed = spectrum.reshape(length, GROUPS * GRP).astype(jnp.bfloat16)
        return jnp.dot(mixed, proj_out, preferred_element_type=jnp.float32).astype(jnp.bfloat16)

    return lax.map(one_sequence, tokens)
```

```python
import math

import jax
import jax.numpy as jnp
import numpy as np
from jax import lax
from jax.experimental import pallas as pl
from jax.experimental.pallas import tpu as pltpu
from jax.sharding import PartitionSpec as P

GRP = 128
LANES = 128
highest = lax.Precision.HIGHEST
span_inner = 128


def circle(height, breadth, period):
    product = lax.iota(jnp.int32, height)[:, None] * lax.iota(jnp.int32, breadth)[None, :] % period
    angle = product.astype(jnp.float32) * (2.0 * math.pi / period)
    return (jnp.cos(angle), jnp.sin(angle))


def positions(piece):
    real_in = piece[0, 0]
    imag_in = piece[1, 0]
    count, length = real_in.shape
    outer = length // span_inner
    real_in = real_in.reshape(count, outer, span_inner)
    imag_in = imag_in.reshape(count, outer, span_inner)
    cos_one, sin_one = circle(outer, outer, outer)
    first_re = jnp.einsum("ab,kbq->kaq", cos_one, real_in, precision=highest) - jnp.einsum(
        "ab,kbq->kaq", sin_one, imag_in, precision=highest
    )
    first_im = jnp.einsum("ab,kbq->kaq", sin_one, real_in, precision=highest) + jnp.einsum(
        "ab,kbq->kaq", cos_one, imag_in, precision=highest
    )
    twist_c, twist_s = circle(outer, span_inner, length)
    turned_re = first_re * twist_c - first_im * twist_s
    turned_im = first_re * twist_s + first_im * twist_c
    cos_two, sin_two = circle(span_inner, span_inner, span_inner)
    factor = 1.0 / math.sqrt(GRP * length)
    real_out = jnp.einsum("kaq,qb->kba", turned_re, cos_two, precision=highest) - jnp.einsum(
        "kaq,qb->kba", turned_im, sin_two, precision=highest
    )
    real_out = real_out.reshape(count, length) * factor
    return real_out[:, None, :]


def general_shards(tokens, proj_in, proj_out):
    seq_rows = tokens[0]
    local_len = seq_rows.shape[0]
    features = proj_in.shape[1]
    groups = features // GRP
    mapped = jnp.dot(
        seq_rows,
        lax.all_gather(proj_in, "col", axis=0, tiled=True),
        preferred_element_type=jnp.float32,
    ).astype(jnp.bfloat16)
    values = mapped.astype(jnp.float32).reshape(local_len, groups, GRP)
    cos_c, sin_c = circle(GRP, GRP, GRP)
    real_part = jnp.einsum("pgc,cs->gsp", values, cos_c, precision=highest)
    imag_part = jnp.einsum("pgc,cs->gsp", values, sin_c, precision=highest)
    ways = lax.axis_size("row")
    slots = groups * cos_c.shape[1]
    per_dev = slots // ways
    stacked = jnp.stack(
        [real_part.reshape(ways, per_dev, local_len), imag_part.reshape(ways, per_dev, local_len)],
        0,
    )
    spectra = positions(lax.all_to_all(stacked, "row", split_axis=1, concat_axis=3, tiled=True))
    outgoing = spectra.astype(jnp.bfloat16)
    back = lax.all_to_all(outgoing, "row", split_axis=2, concat_axis=0, tiled=True)
    mixed = back.reshape(features, local_len)
    result = lax.dot_general(
        mixed,
        lax.all_gather(proj_out, "row", axis=1, tiled=True),
        (((0,), (0,)), ((), ())),
        preferred_element_type=jnp.float32,
    )
    return result.astype(jnp.bfloat16)[None]


def channel_table(quarters, pairs):
    c = np.arange(GRP)
    rows = []
    for t in range(quarters):
        j = pairs * t + np.arange(pairs)
        angle = 2 * np.pi * (j[:, None] * c % GRP) / GRP
        sine = np.sin(angle)
        if t == 0:
            sine[0] = np.cos(np.pi * c)
        rows += [np.cos(angle), sine]
    return np.concatenate(rows, 0)


def channel_order(groups, quarters, pairs):
    order = []
    for g in range(groups):
        for t in range(quarters):
            j = pairs * t + np.arange(pairs)
            mirror = (GRP - j) % GRP
            if t == 0:
                mirror[0] = GRP // 2
            order += list(g * GRP + j) + list(g * GRP + mirror)
    return np.array(order)


def position_tables(ways, span):
    per = span // ways
    q = np.arange(span)
    low = min(LANES, span)
    even = np.zeros((ways, 16, 4 * LANES))
    odd = np.zeros((ways, 16, 4 * LANES))
    for owner in range(ways):
        for m in range(per):
            angle = 2 * np.pi * (q * (per * owner + m) % span) / span
            row = np.zeros(4 * LANES)
            row[:low] = np.cos(angle[:low])
            row[LANES : LANES + low] = np.sin(angle[:low])
            row[2 * LANES : 2 * LANES + span - low] = np.cos(angle[low:])
            row[3 * LANES : 3 * LANES + span - low] = np.sin(angle[low:])
            even[owner, m] = row
            odd[owner, m if m < 8 else m + 4] = row
    return even.reshape(-1, 4 * LANES), odd.reshape(-1, 4 * LANES)


def twiddle_table(ways, span):
    length = ways * span
    factor = 1.0 / math.sqrt(GRP * length)
    q = np.arange(2 * LANES)
    angle = 2 * np.pi * (np.arange(ways)[:, None] * q % length) / length
    cos, sin = np.cos(angle) * factor, np.sin(angle) * factor
    return np.stack([cos[:, :LANES], sin[:, :LANES], cos[:, LANES:], sin[:, LANES:]], 1)


def row_order(span):
    chunk = []
    chunk += [(0, m) for m in range(8)] + [(2, m) for m in range(8)]
    for a in range(4):
        chunk += [((0, 2, 1, 3)[a], 8 + m) for m in range(4)]
    chunk += [(1, m) for m in range(8)] + [(3, m) for m in range(8)]
    rows = len(chunk)
    hot = np.zeros((span, span))
    for b in range(4):
        for i, (a, m) in enumerate(chunk):
            hot[16 * m + 4 * a + b, b * rows + i] = 1
    return hot


def own_kernel(where, tok, w, out):
    out[...] = jnp.dot(tok[...], w[...], preferred_element_type=jnp.float32)


def send_kernel(where, tok, w, part, table, out, padded):
    span, features = part.shape
    mapped = part[...] + jnp.dot(tok[...], w[...], preferred_element_type=jnp.float32)
    padded[pl.ds(0, span), :] = mapped.astype(jnp.bfloat16)
    padded[pl.ds(span, 2 * LANES - span), :] = jnp.zeros((2 * LANES - span, features), jnp.bfloat16)
    groups = features // GRP
    quarters = out.shape[0] // groups
    for g in range(groups):
        turned = lax.dot_general(
            table[...],
            padded[:, g * GRP : (g + 1) * GRP],
            (((1,), (1,)), ((), ())),
            preferred_element_type=jnp.float32,
        )
        for t in range(quarters):
            cos = turned[32 * t : 32 * t + 16]
            sin = turned[32 * t + 16 : 32 * t + 32]
            high = cos[:, LANES:] + pltpu.roll(sin[:, LANES:], LANES // 2, 1)
            d = g * quarters + t
            out[d, 0:16, :] = cos[:, :LANES].astype(jnp.bfloat16)
            out[d, 16:32, :] = sin[:, :LANES].astype(jnp.bfloat16)
            out[d, 32:48, :] = high.astype(jnp.bfloat16)


def fft4(a, b, c, d):
    (ar, ai), (br, bi), (cr, ci), (dr, di) = a, b, c, d
    sr, si, tr, ti = ar + cr, ai + ci, ar - cr, ai - ci
    ur, ui, vr, vi = br + dr, bi + di, br - dr, bi - di
    return [(sr + ur, si + ui), (tr + vi, ti - vr), (sr - ur, si - ui), (tr - vi, ti + vr)]


def turn(v, n):
    re, im = v
    n %= 16
    if n == 0:
        return v
    if n == 4:
        return (im, -re)
    if n == 2:
        h = math.sqrt(0.5)
        return ((re + im) * h, (im - re) * h)
    if n == 6:
        h = math.sqrt(0.5)
        return ((im - re) * h, -(re + im) * h)
    c, s = math.cos(2 * math.pi * n / 16), math.sin(2 * math.pi * n / 16)
    return (re * c + im * s, im * c - re * s)


def fft16(v):
    inner = [fft4(v[a], v[a + 4], v[a + 8], v[a + 12]) for a in range(4)]
    out = [None] * 16
    for f in range(4):
        col = fft4(*[turn(inner[a][f], a * f) for a in range(4)])
        for e in range(4):
            out[f + 4 * e] = col[e]
    return out


def mix_kernel(special, x, even, odd, twist, out, turned):
    ways = x.shape[0]
    first = (lax.broadcasted_iota(jnp.int32, (16, LANES), 0) == 0) & (special[0] == 0)
    for part in range(2):
        v = []
        for r in range(ways):
            if part == 0:
                re = x[r, 0:16, :].astype(jnp.float32)
                im = -x[r, 16:32, :].astype(jnp.float32)
            else:
                re = x[r, 32:48, :].astype(jnp.float32)
                im = -pltpu.roll(re, LANES // 2, 1)
            v.append((re, im))
        spec = fft16(v)
        for k in range(ways):
            pr, pi = spec[k]
            qr, qi = spec[-k % ways]
            qi = -qi
            ur = jnp.where(first, (pr + qr) * 0.5, pr)
            ui = jnp.where(first, (pi + qi) * 0.5, pi)
            wr = jnp.where(first, (qi - pi) * 0.5, qr)
            wi = jnp.where(first, (pr - qr) * 0.5, qi)
            c = twist[k, 2 * part : 2 * part + 1, :]
            s = twist[k, 2 * part + 1 : 2 * part + 2, :]
            lo = slice(2 * part * LANES, (2 * part + 1) * LANES)
            hi = slice((2 * part + 1) * LANES, (2 * part + 2) * LANES)
            turned[32 * k : 32 * k + 16, lo] = (ur * c + ui * s).astype(jnp.bfloat16)
            turned[32 * k : 32 * k + 16, hi] = (ui * c - ur * s).astype(jnp.bfloat16)
            turned[32 * k + 16 : 32 * k + 32, lo] = (wr * c + wi * s).astype(jnp.bfloat16)
            turned[32 * k + 16 : 32 * k + 32, hi] = (wi * c - wr * s).astype(jnp.bfloat16)
    half = turned.shape[0] // 2
    nt = (((1,), (1,)), ((), ()))
    one = lax.dot_general(even[...], turned[:half, :], nt, preferred_element_type=jnp.float32)
    two = lax.dot_general(odd[...], turned[half:, :], nt, preferred_element_type=jnp.float32)
    for r in range(ways):
        e, o = one[16 * r : 16 * r + 16], two[16 * r : 16 * r + 16]
        tail = e[8:] + o[8:]
        left, right = slice(0, LANES), slice(LANES, 2 * LANES)
        out[r, 0:16, :] = jnp.concatenate([e[:8, left], o[:8, left]], 0).astype(jnp.bfloat16)
        out[r, 16:32, :] = jnp.concatenate([tail[:, left], tail[:, right]], 0).astype(jnp.bfloat16)
        out[r, 32:48, :] = jnp.concatenate([e[:8, right], o[:8, right]], 0).astype(jnp.bfloat16)


def gather_blocks(y, groups, stage):
    quarters = y.shape[0] // groups
    rows = y.shape[1]
    lane = lax.broadcasted_iota(jnp.int32, (rows, LANES), 1) // 32
    odd, high = lane % 2 == 1, lane >= 2
    for g in range(groups):
        v = [y[g * quarters + t].astype(jnp.float32) for t in range(quarters)]
        w = [None] * 4
        for t in (0, 2):
            w[t] = jnp.where(odd, pltpu.roll(v[t + 1], 32, 1), v[t])
            w[t + 1] = jnp.where(odd, v[t + 1], pltpu.roll(v[t], LANES - 32, 1))
        u = [None] * 4
        for b in (0, 1):
            u[b] = jnp.where(high, pltpu.roll(w[b + 2], 64, 1), w[b])
            u[b + 2] = jnp.where(high, w[b + 2], pltpu.roll(w[b], 64, 1))
        for b in range(4):
            stage[b * rows : (b + 1) * rows, g * GRP : (g + 1) * GRP] = u[b].astype(jnp.bfloat16)


def out_kernel(y, hot, w, out, stage):
    groups = w.shape[0] // GRP
    gather_blocks(y, groups, stage)
    mixed = jnp.dot(hot[...], stage[...], preferred_element_type=jnp.float32).astype(jnp.bfloat16)
    out[...] = jnp.dot(mixed, w[...], preferred_element_type=jnp.float32).astype(jnp.bfloat16)


def vmem(count):
    return [pl.BlockSpec(memory_space=pltpu.VMEM)] * count


def shards(tokens, proj_in, proj_out):
    seq_rows = tokens[0]
    span, width = seq_rows.shape
    depth, features = proj_in.shape
    ways = lax.axis_size("row")
    groups = features // GRP
    quarters = ways // groups
    pairs = GRP // 2 // quarters
    bf16, f32 = jnp.bfloat16, jnp.float32

    order = channel_order(groups, quarters, pairs)
    hot_w = np.zeros((groups, GRP, GRP))
    for g in range(groups):
        hot_w[g, np.arange(GRP), order[g * GRP : (g + 1) * GRP] - g * GRP] = 1
    w_out = jnp.einsum(
        "gab,gbn->gan", jnp.asarray(hot_w, bf16), proj_out.reshape(groups, GRP, -1), preferred_element_type=f32
    ).astype(bf16)
    w_out = lax.all_gather(w_out.reshape(features, -1), "row", axis=1, tiled=True)

    me = lax.axis_index("col")
    other_w = lax.ppermute(proj_in, "col", [(0, 1), (1, 0)])
    tok_spec = lambda pick: pl.BlockSpec((span, depth), pick)
    whole = lambda shape: pl.BlockSpec(shape, lambda i, s: (0,) * len(shape))
    part = pl.pallas_call(
        own_kernel,
        grid_spec=pltpu.PrefetchScalarGridSpec(
            num_scalar_prefetch=1,
            grid=(1,),
            in_specs=[tok_spec(lambda i, s: (0, s[0])), whole((depth, features))],
            out_specs=whole((span, features)),
        ),
        out_shape=jax.ShapeDtypeStruct((span, features), f32),
        cost_estimate=pl.CostEstimate(flops=2 * span * depth * features, bytes_accessed=2 << 20, transcendentals=0),
        name="own_half",
    )(me[None], seq_rows, proj_in)
    table = jnp.asarray(channel_table(quarters, pairs), bf16)
    sent = pl.pallas_call(
        send_kernel,
        grid_spec=pltpu.PrefetchScalarGridSpec(
            num_scalar_prefetch=1,
            grid=(1,),
            in_specs=[
                tok_spec(lambda i, s: (0, s[0])),
                whole((depth, features)),
                whole((span, features)),
                whole(table.shape),
            ],
            out_specs=whole((ways, 48, LANES)),
            scratch_shapes=[pltpu.VMEM((2 * LANES, features), bf16)],
        ),
        out_shape=jax.ShapeDtypeStruct((ways, 48, LANES), bf16),
        cost_estimate=pl.CostEstimate(flops=2 * span * depth * features, bytes_accessed=2 << 20, transcendentals=0),
        name="send",
    )((1 - me)[None], seq_rows, other_w, part, table)

    held = lax.all_to_all(sent, "row", 0, 0, tiled=True)

    even, odd = position_tables(ways, span)
    even, odd = jnp.asarray(even, bf16), jnp.asarray(odd, bf16)
    twist = jnp.asarray(twiddle_table(ways, span), f32)
    special = lax.rem(lax.axis_index("row"), quarters)[None]
    spectra = pl.pallas_call(
        mix_kernel,
        in_specs=[pl.BlockSpec(memory_space=pltpu.SMEM)] + vmem(4),
        out_specs=vmem(1)[0],
        out_shape=jax.ShapeDtypeStruct((ways, 48, LANES), bf16),
        scratch_shapes=[pltpu.VMEM((ways * 32, 4 * LANES), bf16)],
        name="mix",
    )(special, held, even, odd, twist)

    back = lax.all_to_all(spectra, "row", 0, 0, tiled=True)

    hot = jnp.asarray(row_order(span), bf16)
    result = pl.pallas_call(
        out_kernel,
        in_specs=vmem(3),
        out_specs=vmem(1)[0],
        out_shape=jax.ShapeDtypeStruct((span, w_out.shape[1]), bf16),
        scratch_shapes=[pltpu.VMEM((span, features), bf16)],
        name="out",
    )(back, hot, w_out)
    return result[None]


def fits(mesh, tokens, proj_in, proj_out):
    ways, cols = mesh.shape["row"], mesh.shape["col"]
    features = proj_in.shape[1]
    span = tokens.shape[1] // ways
    return (
        features % GRP == 0
        and ways == 4 * (features // GRP) == 16
        and span == 12 * ways
        and cols == 2
        and tokens.shape[0] == cols
        and proj_out.shape[1] % (ways * LANES) == 0
    )


def solution(mesh):
    in_specs = (P("col", "row", None), P("col", None), P(None, "row"))
    out_specs = P("col", "row", None)

    def run(tokens, proj_in, proj_out):
        body = shards if fits(mesh, tokens, proj_in, proj_out) else general_shards
        return jax.shard_map(body, mesh=mesh, in_specs=in_specs, out_specs=out_specs, check_vma=False)(
            tokens, proj_in, proj_out
        )

    return run
```

```python
import math

import jax
import jax.numpy as jnp
import numpy as np
from jax import lax
from jax.experimental import pallas as pl
from jax.experimental.pallas import tpu as pltpu
from jax.sharding import PartitionSpec as P

GRP = 128
LANES = 128
highest = lax.Precision.HIGHEST
span_inner = 128


def circle(height, breadth, period):
    product = lax.iota(jnp.int32, height)[:, None] * lax.iota(jnp.int32, breadth)[None, :] % period
    angle = product.astype(jnp.float32) * (2.0 * math.pi / period)
    return (jnp.cos(angle), jnp.sin(angle))


def positions(piece):
    real_in = piece[0, 0]
    imag_in = piece[1, 0]
    count, length = real_in.shape
    outer = length // span_inner
    real_in = real_in.reshape(count, outer, span_inner)
    imag_in = imag_in.reshape(count, outer, span_inner)
    cos_one, sin_one = circle(outer, outer, outer)
    first_re = jnp.einsum("ab,kbq->kaq", cos_one, real_in, precision=highest) - jnp.einsum(
        "ab,kbq->kaq", sin_one, imag_in, precision=highest
    )
    first_im = jnp.einsum("ab,kbq->kaq", sin_one, real_in, precision=highest) + jnp.einsum(
        "ab,kbq->kaq", cos_one, imag_in, precision=highest
    )
    twist_c, twist_s = circle(outer, span_inner, length)
    turned_re = first_re * twist_c - first_im * twist_s
    turned_im = first_re * twist_s + first_im * twist_c
    cos_two, sin_two = circle(span_inner, span_inner, span_inner)
    factor = 1.0 / math.sqrt(GRP * length)
    real_out = jnp.einsum("kaq,qb->kba", turned_re, cos_two, precision=highest) - jnp.einsum(
        "kaq,qb->kba", turned_im, sin_two, precision=highest
    )
    real_out = real_out.reshape(count, length) * factor
    return real_out[:, None, :]


def general_shards(tokens, proj_in, proj_out):
    seq_rows = tokens[0]
    local_len = seq_rows.shape[0]
    features = proj_in.shape[1]
    groups = features // GRP
    mapped = jnp.dot(
        seq_rows,
        lax.all_gather(proj_in, "col", axis=0, tiled=True),
        preferred_element_type=jnp.float32,
    ).astype(jnp.bfloat16)
    values = mapped.astype(jnp.float32).reshape(local_len, groups, GRP)
    cos_c, sin_c = circle(GRP, GRP, GRP)
    real_part = jnp.einsum("pgc,cs->gsp", values, cos_c, precision=highest)
    imag_part = jnp.einsum("pgc,cs->gsp", values, sin_c, precision=highest)
    ways = lax.axis_size("row")
    slots = groups * cos_c.shape[1]
    per_dev = slots // ways
    stacked = jnp.stack(
        [real_part.reshape(ways, per_dev, local_len), imag_part.reshape(ways, per_dev, local_len)],
        0,
    )
    spectra = positions(lax.all_to_all(stacked, "row", split_axis=1, concat_axis=3, tiled=True))
    outgoing = spectra.astype(jnp.bfloat16)
    back = lax.all_to_all(outgoing, "row", split_axis=2, concat_axis=0, tiled=True)
    mixed = back.reshape(features, local_len)
    result = lax.dot_general(
        mixed,
        lax.all_gather(proj_out, "row", axis=1, tiled=True),
        (((0,), (0,)), ((), ())),
        preferred_element_type=jnp.float32,
    )
    return result.astype(jnp.bfloat16)[None]


def channel_table(quarters, pairs):
    c = np.arange(GRP)
    rows = []
    for t in range(quarters):
        j = pairs * t + np.arange(pairs)
        angle = 2 * np.pi * (j[:, None] * c % GRP) / GRP
        sine = np.sin(angle)
        if t == 0:
            sine[0] = np.cos(np.pi * c)
        rows += [np.cos(angle), sine]
    return np.concatenate(rows, 0)


def channel_order(groups, quarters, pairs):
    order = []
    for g in range(groups):
        for t in range(quarters):
            j = pairs * t + np.arange(pairs)
            mirror = (GRP - j) % GRP
            if t == 0:
                mirror[0] = GRP // 2
            order += list(g * GRP + j) + list(g * GRP + mirror)
    return np.array(order)


def position_tables(ways, span):
    per = span // ways
    q = np.arange(span)
    low = min(LANES, span)
    even = np.zeros((ways, 16, 4 * LANES))
    odd = np.zeros((ways, 16, 4 * LANES))
    for owner in range(ways):
        for m in range(per):
            angle = 2 * np.pi * (q * (per * owner + m) % span) / span
            row = np.zeros(4 * LANES)
            row[:low] = np.cos(angle[:low])
            row[LANES : LANES + low] = np.sin(angle[:low])
            row[2 * LANES : 2 * LANES + span - low] = np.cos(angle[low:])
            row[3 * LANES : 3 * LANES + span - low] = np.sin(angle[low:])
            even[owner, m] = row
            odd[owner, m if m < 8 else m + 4] = row
    return even.reshape(-1, 4 * LANES), odd.reshape(-1, 4 * LANES)


def twiddle_table(ways, span):
    length = ways * span
    factor = 1.0 / math.sqrt(GRP * length)
    q = np.arange(2 * LANES)
    angle = 2 * np.pi * (np.arange(ways)[:, None] * q % length) / length
    cos, sin = np.cos(angle) * factor, np.sin(angle) * factor
    return np.stack([cos[:, :LANES], sin[:, :LANES], cos[:, LANES:], sin[:, LANES:]], 1)


def row_order(span):
    chunk = []
    chunk += [(0, m) for m in range(8)] + [(2, m) for m in range(8)]
    for a in range(4):
        chunk += [((0, 2, 1, 3)[a], 8 + m) for m in range(4)]
    chunk += [(1, m) for m in range(8)] + [(3, m) for m in range(8)]
    rows = len(chunk)
    hot = np.zeros((span, span))
    for b in range(4):
        for i, (a, m) in enumerate(chunk):
            hot[16 * m + 4 * a + b, b * rows + i] = 1
    return hot


def own_kernel(where, tok, w, out):
    out[...] = jnp.dot(tok[...], w[...], preferred_element_type=jnp.float32)


def send_kernel(where, tok, w, part, table, out, padded):
    span, features = part.shape
    mapped = part[...] + jnp.dot(tok[...], w[...], preferred_element_type=jnp.float32)
    padded[pl.ds(0, span), :] = mapped.astype(jnp.bfloat16)
    padded[pl.ds(span, 2 * LANES - span), :] = jnp.zeros((2 * LANES - span, features), jnp.bfloat16)
    groups = features // GRP
    quarters = out.shape[0] // groups
    for g in range(groups):
        turned = lax.dot_general(
            table[...],
            padded[:, g * GRP : (g + 1) * GRP],
            (((1,), (1,)), ((), ())),
            preferred_element_type=jnp.float32,
        )
        for t in range(quarters):
            cos = turned[32 * t : 32 * t + 16]
            sin = turned[32 * t + 16 : 32 * t + 32]
            high = cos[:, LANES:] + pltpu.roll(sin[:, LANES:], LANES // 2, 1)
            d = g * quarters + t
            out[d, 0:16, :] = cos[:, :LANES].astype(jnp.bfloat16)
            out[d, 16:32, :] = sin[:, :LANES].astype(jnp.bfloat16)
            out[d, 32:48, :] = high.astype(jnp.bfloat16)


def fft4(a, b, c, d):
    (ar, ai), (br, bi), (cr, ci), (dr, di) = a, b, c, d
    sr, si, tr, ti = ar + cr, ai + ci, ar - cr, ai - ci
    ur, ui, vr, vi = br + dr, bi + di, br - dr, bi - di
    return [(sr + ur, si + ui), (tr + vi, ti - vr), (sr - ur, si - ui), (tr - vi, ti + vr)]


def turn(v, n):
    re, im = v
    n %= 16
    if n == 0:
        return v
    if n == 4:
        return (im, -re)
    if n == 2:
        h = math.sqrt(0.5)
        return ((re + im) * h, (im - re) * h)
    if n == 6:
        h = math.sqrt(0.5)
        return ((im - re) * h, -(re + im) * h)
    c, s = math.cos(2 * math.pi * n / 16), math.sin(2 * math.pi * n / 16)
    return (re * c + im * s, im * c - re * s)


def fft16(v):
    inner = [fft4(v[a], v[a + 4], v[a + 8], v[a + 12]) for a in range(4)]
    out = [None] * 16
    for f in range(4):
        col = fft4(*[turn(inner[a][f], a * f) for a in range(4)])
        for e in range(4):
            out[f + 4 * e] = col[e]
    return out


def mix_kernel(special, x, even, odd, twist, out, turned):
    ways = x.shape[0]
    first = (lax.broadcasted_iota(jnp.int32, (16, LANES), 0) == 0) & (special[0] == 0)
    for part in range(2):
        v = []
        for r in range(ways):
            if part == 0:
                re = x[r, 0:16, :].astype(jnp.float32)
                im = -x[r, 16:32, :].astype(jnp.float32)
            else:
                re = x[r, 32:48, :].astype(jnp.float32)
                im = -pltpu.roll(re, LANES // 2, 1)
            v.append((re, im))
        spec = fft16(v)
        for k in range(ways):
            pr, pi = spec[k]
            qr, qi = spec[-k % ways]
            qi = -qi
            ur = jnp.where(first, (pr + qr) * 0.5, pr)
            ui = jnp.where(first, (pi + qi) * 0.5, pi)
            wr = jnp.where(first, (qi - pi) * 0.5, qr)
            wi = jnp.where(first, (pr - qr) * 0.5, qi)
            c = twist[k, 2 * part : 2 * part + 1, :]
            s = twist[k, 2 * part + 1 : 2 * part + 2, :]
            lo = slice(2 * part * LANES, (2 * part + 1) * LANES)
            hi = slice((2 * part + 1) * LANES, (2 * part + 2) * LANES)
            turned[32 * k : 32 * k + 16, lo] = (ur * c + ui * s).astype(jnp.bfloat16)
            turned[32 * k : 32 * k + 16, hi] = (ui * c - ur * s).astype(jnp.bfloat16)
            turned[32 * k + 16 : 32 * k + 32, lo] = (wr * c + wi * s).astype(jnp.bfloat16)
            turned[32 * k + 16 : 32 * k + 32, hi] = (wi * c - wr * s).astype(jnp.bfloat16)
    half = turned.shape[0] // 2
    nt = (((1,), (1,)), ((), ()))
    one = lax.dot_general(even[...], turned[:half, :], nt, preferred_element_type=jnp.float32)
    two = lax.dot_general(odd[...], turned[half:, :], nt, preferred_element_type=jnp.float32)
    for r in range(ways):
        e, o = one[16 * r : 16 * r + 16], two[16 * r : 16 * r + 16]
        tail = e[8:] + o[8:]
        left, right = slice(0, LANES), slice(LANES, 2 * LANES)
        out[r, 0:16, :] = jnp.concatenate([e[:8, left], o[:8, left]], 0).astype(jnp.bfloat16)
        out[r, 16:32, :] = jnp.concatenate([tail[:, left], tail[:, right]], 0).astype(jnp.bfloat16)
        out[r, 32:48, :] = jnp.concatenate([e[:8, right], o[:8, right]], 0).astype(jnp.bfloat16)


def gather_blocks(y, groups, stage):
    quarters = y.shape[0] // groups
    rows = y.shape[1]
    lane = lax.broadcasted_iota(jnp.int32, (rows, LANES), 1) // 32
    odd, high = lane % 2 == 1, lane >= 2
    for g in range(groups):
        v = [y[g * quarters + t].astype(jnp.float32) for t in range(quarters)]
        w = [None] * 4
        for t in (0, 2):
            w[t] = jnp.where(odd, pltpu.roll(v[t + 1], 32, 1), v[t])
            w[t + 1] = jnp.where(odd, v[t + 1], pltpu.roll(v[t], LANES - 32, 1))
        u = [None] * 4
        for b in (0, 1):
            u[b] = jnp.where(high, pltpu.roll(w[b + 2], 64, 1), w[b])
            u[b + 2] = jnp.where(high, w[b + 2], pltpu.roll(w[b], 64, 1))
        for b in range(4):
            stage[b * rows : (b + 1) * rows, g * GRP : (g + 1) * GRP] = u[b].astype(jnp.bfloat16)


def out_kernel(place, y, hot, swap, near_own, near_other, far_own, far_other, out, stage, mixed):
    row, core = place[0], place[1]
    features = stage.shape[1]
    groups = features // GRP
    half = features // 2
    gather_blocks(y, groups, stage)
    rows = jnp.dot(hot[...], stage[...], preferred_element_type=jnp.float32).astype(jnp.bfloat16)
    for g in range(groups):
        part = slice(g * GRP, (g + 1) * GRP)
        mixed[:, part] = jnp.dot(rows[:, part], swap[...], preferred_element_type=jnp.float32).astype(jnp.bfloat16)
    own = mixed[:, pl.ds(pl.multiple_of(core * half, half), half)]
    other = mixed[:, pl.ds(pl.multiple_of((1 - core) * half, half), half)]
    ways = 2 * near_own.shape[0]
    for dx, (left, right) in enumerate(((near_own, near_other), (far_own, far_other))):
        for i in range(0, ways // 2, 2):
            both = jnp.dot(
                own, jnp.concatenate([left[i], left[i + 1]], 1), preferred_element_type=jnp.float32
            ) + jnp.dot(other, jnp.concatenate([right[i], right[i + 1]], 1), preferred_element_type=jnp.float32)
            for n in range(2):
                dy, dz = (i + n) // (ways // 4), (i + n) % (ways // 4)
                owner = relative(row, ways, dx, dy, dz)
                out[:, pl.ds(pl.multiple_of(owner * LANES, LANES), LANES)] = both[
                    :, n * LANES : (n + 1) * LANES
                ].astype(jnp.bfloat16)


def relative(row, ways, dx, dy, dz):
    x, y = lax.rem(row, 2), lax.rem(lax.div(row, 2), 2)
    x = 1 - x if dx else x
    y = 1 - y if dy else y
    return lax.rem(lax.div(row, 4) * 4 + 4 * dz, ways) + 2 * y + x


def vmem(count):
    return [pl.BlockSpec(memory_space=pltpu.VMEM)] * count


def shards(tokens, proj_in, proj_out):
    seq_rows = tokens[0]
    span, width = seq_rows.shape
    depth, features = proj_in.shape
    ways = lax.axis_size("row")
    groups = features // GRP
    quarters = ways // groups
    pairs = GRP // 2 // quarters
    bf16, f32 = jnp.bfloat16, jnp.float32
    room = pltpu.CompilerParams(vmem_limit_bytes=16 << 20)

    me = lax.axis_index("col")
    swap_cores = lambda v: lax.ppermute(v, "col", [(0, 1), (1, 0)])
    other_w = swap_cores(proj_in)
    half = features // 2
    mine = lax.dynamic_slice_in_dim(proj_out, me * half, half, 0)
    along = lambda v, to: lax.ppermute(v, "row", [(i, to(i)) for i in range(ways)])
    ring = [mine]
    for dz in range(1, ways // 4):
        ring.append(along(mine, lambda i: (i - 4 * dz) % ways))
    ring = jnp.stack(ring, 0)
    tok_spec = lambda pick: pl.BlockSpec((span, depth), pick)
    whole = lambda shape: pl.BlockSpec(shape, lambda i, s: (0,) * len(shape))
    part = pl.pallas_call(
        own_kernel,
        grid_spec=pltpu.PrefetchScalarGridSpec(
            num_scalar_prefetch=1,
            grid=(1,),
            in_specs=[tok_spec(lambda i, s: (0, s[0])), whole((depth, features))],
            out_specs=whole((span, features)),
        ),
        out_shape=jax.ShapeDtypeStruct((span, features), f32),
        cost_estimate=pl.CostEstimate(flops=2 * span * depth * features, bytes_accessed=2 << 20, transcendentals=0),
        compiler_params=room,
        name="own_half",
    )(me[None], seq_rows, proj_in)
    table = jnp.asarray(channel_table(quarters, pairs), bf16)
    sent = pl.pallas_call(
        send_kernel,
        grid_spec=pltpu.PrefetchScalarGridSpec(
            num_scalar_prefetch=1,
            grid=(1,),
            in_specs=[
                tok_spec(lambda i, s: (0, s[0])),
                whole((depth, features)),
                whole((span, features)),
                whole(table.shape),
            ],
            out_specs=whole((ways, 48, LANES)),
            scratch_shapes=[pltpu.VMEM((2 * LANES, features), bf16)],
        ),
        out_shape=jax.ShapeDtypeStruct((ways, 48, LANES), bf16),
        cost_estimate=pl.CostEstimate(flops=2 * span * depth * features, bytes_accessed=2 << 20, transcendentals=0),
        compiler_params=room,
        name="send",
    )((1 - me)[None], seq_rows, other_w, part, table)

    sent, ring = lax.optimization_barrier((sent, ring))
    plane = along(ring, lambda i: i ^ 2)
    held = lax.all_to_all(sent, "row", 0, 0, tiled=True)
    held, plane = lax.optimization_barrier((held, plane))
    near = jnp.concatenate([ring, plane], 0)
    far = along(near, lambda i: i ^ 1)
    near_other = swap_cores(near)

    even, odd = position_tables(ways, span)
    even, odd = jnp.asarray(even, bf16), jnp.asarray(odd, bf16)
    twist = jnp.asarray(twiddle_table(ways, span), f32)
    special = lax.rem(lax.axis_index("row"), quarters)[None]
    spectra = pl.pallas_call(
        mix_kernel,
        in_specs=[pl.BlockSpec(memory_space=pltpu.SMEM)] + vmem(4),
        out_specs=vmem(1)[0],
        out_shape=jax.ShapeDtypeStruct((ways, 48, LANES), bf16),
        scratch_shapes=[pltpu.VMEM((ways * 32, 4 * LANES), bf16)],
        compiler_params=room,
        name="mix",
    )(special, held, even, odd, twist)

    back = lax.all_to_all(spectra, "row", 0, 0, tiled=True)

    back, far = lax.optimization_barrier((back, far))
    far_other = swap_cores(far)
    hot = jnp.asarray(row_order(span), bf16)
    swap = np.zeros((GRP, GRP))
    swap[np.arange(GRP), channel_order(1, quarters, pairs)] = 1
    place = jnp.stack([lax.axis_index("row"), me])
    result = pl.pallas_call(
        out_kernel,
        in_specs=[pl.BlockSpec(memory_space=pltpu.SMEM)] + vmem(7),
        out_specs=vmem(1)[0],
        out_shape=jax.ShapeDtypeStruct((span, ways * LANES), bf16),
        scratch_shapes=[pltpu.VMEM((span, features), bf16)] * 2,
        compiler_params=room,
        name="out",
    )(place, back, hot, jnp.asarray(swap, bf16), near, near_other, far, far_other)
    return result[None]


def fits(mesh, tokens, proj_in, proj_out):
    ways, cols = mesh.shape["row"], mesh.shape["col"]
    features = proj_in.shape[1]
    span = tokens.shape[1] // ways
    return (
        features % GRP == 0
        and ways == 4 * (features // GRP) == 16
        and span == 12 * ways
        and cols == 2
        and tokens.shape[0] == cols
        and proj_out.shape[1] == ways * LANES
    )


def solution(mesh):
    in_specs = (P("col", "row", None), P("col", None), P(None, "row"))
    out_specs = P("col", "row", None)

    def run(tokens, proj_in, proj_out):
        body = shards if fits(mesh, tokens, proj_in, proj_out) else general_shards
        return jax.shard_map(body, mesh=mesh, in_specs=in_specs, out_specs=out_specs, check_vma=False)(
            tokens, proj_in, proj_out
        )

    return run
```

```python
import math

import jax
import jax.numpy as jnp
import numpy as np
from jax import lax
from jax.experimental import pallas as pl
from jax.experimental.pallas import tpu as pltpu
from jax.sharding import PartitionSpec as P

GRP = 128
LANES = 128
highest = lax.Precision.HIGHEST
span_inner = 128


def circle(height, breadth, period):
    product = lax.iota(jnp.int32, height)[:, None] * lax.iota(jnp.int32, breadth)[None, :] % period
    angle = product.astype(jnp.float32) * (2.0 * math.pi / period)
    return (jnp.cos(angle), jnp.sin(angle))


def positions(piece):
    real_in = piece[0, 0]
    imag_in = piece[1, 0]
    count, length = real_in.shape
    outer = length // span_inner
    real_in = real_in.reshape(count, outer, span_inner)
    imag_in = imag_in.reshape(count, outer, span_inner)
    cos_one, sin_one = circle(outer, outer, outer)
    first_re = jnp.einsum("ab,kbq->kaq", cos_one, real_in, precision=highest) - jnp.einsum(
        "ab,kbq->kaq", sin_one, imag_in, precision=highest
    )
    first_im = jnp.einsum("ab,kbq->kaq", sin_one, real_in, precision=highest) + jnp.einsum(
        "ab,kbq->kaq", cos_one, imag_in, precision=highest
    )
    twist_c, twist_s = circle(outer, span_inner, length)
    turned_re = first_re * twist_c - first_im * twist_s
    turned_im = first_re * twist_s + first_im * twist_c
    cos_two, sin_two = circle(span_inner, span_inner, span_inner)
    factor = 1.0 / math.sqrt(GRP * length)
    real_out = jnp.einsum("kaq,qb->kba", turned_re, cos_two, precision=highest) - jnp.einsum(
        "kaq,qb->kba", turned_im, sin_two, precision=highest
    )
    real_out = real_out.reshape(count, length) * factor
    return real_out[:, None, :]


def general_shards(tokens, proj_in, proj_out):
    seq_rows = tokens[0]
    local_len = seq_rows.shape[0]
    features = proj_in.shape[1]
    groups = features // GRP
    mapped = jnp.dot(
        seq_rows,
        lax.all_gather(proj_in, "col", axis=0, tiled=True),
        preferred_element_type=jnp.float32,
    ).astype(jnp.bfloat16)
    values = mapped.astype(jnp.float32).reshape(local_len, groups, GRP)
    cos_c, sin_c = circle(GRP, GRP, GRP)
    real_part = jnp.einsum("pgc,cs->gsp", values, cos_c, precision=highest)
    imag_part = jnp.einsum("pgc,cs->gsp", values, sin_c, precision=highest)
    ways = lax.axis_size("row")
    slots = groups * cos_c.shape[1]
    per_dev = slots // ways
    stacked = jnp.stack(
        [real_part.reshape(ways, per_dev, local_len), imag_part.reshape(ways, per_dev, local_len)],
        0,
    )
    spectra = positions(lax.all_to_all(stacked, "row", split_axis=1, concat_axis=3, tiled=True))
    outgoing = spectra.astype(jnp.bfloat16)
    back = lax.all_to_all(outgoing, "row", split_axis=2, concat_axis=0, tiled=True)
    mixed = back.reshape(features, local_len)
    result = lax.dot_general(
        mixed,
        lax.all_gather(proj_out, "row", axis=1, tiled=True),
        (((0,), (0,)), ((), ())),
        preferred_element_type=jnp.float32,
    )
    return result.astype(jnp.bfloat16)[None]


def channel_table(quarters, pairs):
    c = np.arange(GRP)
    rows = []
    for t in range(quarters):
        j = pairs * t + np.arange(pairs)
        angle = 2 * np.pi * (j[:, None] * c % GRP) / GRP
        sine = np.sin(angle)
        if t == 0:
            sine[0] = np.cos(np.pi * c)
        rows += [np.cos(angle), sine]
    return np.concatenate(rows, 0)


def channel_order(groups, quarters, pairs):
    order = []
    for g in range(groups):
        for t in range(quarters):
            j = pairs * t + np.arange(pairs)
            mirror = (GRP - j) % GRP
            if t == 0:
                mirror[0] = GRP // 2
            order += list(g * GRP + j) + list(g * GRP + mirror)
    return np.array(order)


def position_tables(ways, span):
    per = span // ways
    q = np.arange(span)
    low = min(LANES, span)
    even = np.zeros((ways, 16, 4 * LANES))
    odd = np.zeros((ways, 16, 4 * LANES))
    for owner in range(ways):
        for m in range(per):
            angle = 2 * np.pi * (q * (per * owner + m) % span) / span
            row = np.zeros(4 * LANES)
            row[:low] = np.cos(angle[:low])
            row[LANES : LANES + low] = np.sin(angle[:low])
            row[2 * LANES : 2 * LANES + span - low] = np.cos(angle[low:])
            row[3 * LANES : 3 * LANES + span - low] = np.sin(angle[low:])
            even[owner, m] = row
            odd[owner, m if m < 8 else m + 4] = row
    return even.reshape(-1, 4 * LANES), odd.reshape(-1, 4 * LANES)


def twiddle_table(ways, span):
    length = ways * span
    factor = 1.0 / math.sqrt(GRP * length)
    q = np.arange(2 * LANES)
    angle = 2 * np.pi * (np.arange(ways)[:, None] * q % length) / length
    cos, sin = np.cos(angle) * factor, np.sin(angle) * factor
    return np.stack([cos[:, :LANES], sin[:, :LANES], cos[:, LANES:], sin[:, LANES:]], 1)


def row_order(span):
    chunk = []
    chunk += [(0, m) for m in range(8)] + [(2, m) for m in range(8)]
    for a in range(4):
        chunk += [((0, 2, 1, 3)[a], 8 + m) for m in range(4)]
    chunk += [(1, m) for m in range(8)] + [(3, m) for m in range(8)]
    rows = len(chunk)
    hot = np.zeros((span, span))
    for b in range(4):
        for i, (a, m) in enumerate(chunk):
            hot[16 * m + 4 * a + b, b * rows + i] = 1
    return hot


def own_kernel(core, tok, w, table, w_out, part, tok_other, table_copy, mine, tok_own, w_own, sems):
    depth = w_own.shape[0]
    half = mine.shape[0]
    me = core[0]
    columns = lambda which: pl.ds(pl.multiple_of(which * depth, depth), depth)
    copies = [
        pltpu.make_async_copy(tok.at[:, columns(me)], tok_own, sems.at[0]),
        pltpu.make_async_copy(w, w_own, sems.at[1]),
        pltpu.make_async_copy(w_out.at[pl.ds(pl.multiple_of(me * half, half), half), :], mine, sems.at[2]),
        pltpu.make_async_copy(tok.at[:, columns(1 - me)], tok_other, sems.at[3]),
        pltpu.make_async_copy(table, table_copy, sems.at[4]),
    ]
    for copy in copies:
        copy.start()
    copies[0].wait()
    copies[1].wait()
    part[...] = jnp.dot(tok_own[...], w_own[...], preferred_element_type=jnp.float32)
    for copy in copies[2:]:
        copy.wait()


def send_kernel(tok, w, part, table, out, padded):
    span, features = part.shape
    mapped = part[...] + jnp.dot(tok[...], w[...], preferred_element_type=jnp.float32)
    padded[pl.ds(0, span), :] = mapped.astype(jnp.bfloat16)
    padded[pl.ds(span, 2 * LANES - span), :] = jnp.zeros((2 * LANES - span, features), jnp.bfloat16)
    groups = features // GRP
    quarters = out.shape[0] // groups
    for g in range(groups):
        turned = lax.dot_general(
            table[...],
            padded[:, g * GRP : (g + 1) * GRP],
            (((1,), (1,)), ((), ())),
            preferred_element_type=jnp.float32,
        )
        for t in range(quarters):
            cos = turned[32 * t : 32 * t + 16]
            sin = turned[32 * t + 16 : 32 * t + 32]
            high = cos[:, LANES:] + pltpu.roll(sin[:, LANES:], LANES // 2, 1)
            d = g * quarters + t
            out[d, 0:16, :] = cos[:, :LANES].astype(jnp.bfloat16)
            out[d, 16:32, :] = sin[:, :LANES].astype(jnp.bfloat16)
            out[d, 32:48, :] = high.astype(jnp.bfloat16)


def fft4(a, b, c, d):
    (ar, ai), (br, bi), (cr, ci), (dr, di) = a, b, c, d
    sr, si, tr, ti = ar + cr, ai + ci, ar - cr, ai - ci
    ur, ui, vr, vi = br + dr, bi + di, br - dr, bi - di
    return [(sr + ur, si + ui), (tr + vi, ti - vr), (sr - ur, si - ui), (tr - vi, ti + vr)]


def turn(v, n):
    re, im = v
    n %= 16
    if n == 0:
        return v
    if n == 4:
        return (im, -re)
    if n == 2:
        h = math.sqrt(0.5)
        return ((re + im) * h, (im - re) * h)
    if n == 6:
        h = math.sqrt(0.5)
        return ((im - re) * h, -(re + im) * h)
    c, s = math.cos(2 * math.pi * n / 16), math.sin(2 * math.pi * n / 16)
    return (re * c + im * s, im * c - re * s)


def fft16(v):
    inner = [fft4(v[a], v[a + 4], v[a + 8], v[a + 12]) for a in range(4)]
    out = [None] * 16
    for f in range(4):
        col = fft4(*[turn(inner[a][f], a * f) for a in range(4)])
        for e in range(4):
            out[f + 4 * e] = col[e]
    return out


def mix_kernel(special, x, even, odd, twist, out, turned):
    ways = x.shape[0]
    first = (lax.broadcasted_iota(jnp.int32, (16, LANES), 0) == 0) & (special[0] == 0)
    for part in range(2):
        v = []
        for r in range(ways):
            if part == 0:
                re = x[r, 0:16, :].astype(jnp.float32)
                im = -x[r, 16:32, :].astype(jnp.float32)
            else:
                re = x[r, 32:48, :].astype(jnp.float32)
                im = -pltpu.roll(re, LANES // 2, 1)
            v.append((re, im))
        spec = fft16(v)
        for k in range(ways):
            pr, pi = spec[k]
            qr, qi = spec[-k % ways]
            qi = -qi
            ur = jnp.where(first, (pr + qr) * 0.5, pr)
            ui = jnp.where(first, (pi + qi) * 0.5, pi)
            wr = jnp.where(first, (qi - pi) * 0.5, qr)
            wi = jnp.where(first, (pr - qr) * 0.5, qi)
            c = twist[k, 2 * part : 2 * part + 1, :]
            s = twist[k, 2 * part + 1 : 2 * part + 2, :]
            lo = slice(2 * part * LANES, (2 * part + 1) * LANES)
            hi = slice((2 * part + 1) * LANES, (2 * part + 2) * LANES)
            turned[32 * k : 32 * k + 16, lo] = (ur * c + ui * s).astype(jnp.bfloat16)
            turned[32 * k : 32 * k + 16, hi] = (ui * c - ur * s).astype(jnp.bfloat16)
            turned[32 * k + 16 : 32 * k + 32, lo] = (wr * c + wi * s).astype(jnp.bfloat16)
            turned[32 * k + 16 : 32 * k + 32, hi] = (wi * c - wr * s).astype(jnp.bfloat16)
    half = turned.shape[0] // 2
    nt = (((1,), (1,)), ((), ()))
    one = lax.dot_general(even[...], turned[:half, :], nt, preferred_element_type=jnp.float32)
    two = lax.dot_general(odd[...], turned[half:, :], nt, preferred_element_type=jnp.float32)
    for r in range(ways):
        e, o = one[16 * r : 16 * r + 16], two[16 * r : 16 * r + 16]
        tail = e[8:] + o[8:]
        left, right = slice(0, LANES), slice(LANES, 2 * LANES)
        out[r, 0:16, :] = jnp.concatenate([e[:8, left], o[:8, left]], 0).astype(jnp.bfloat16)
        out[r, 16:32, :] = jnp.concatenate([tail[:, left], tail[:, right]], 0).astype(jnp.bfloat16)
        out[r, 32:48, :] = jnp.concatenate([e[:8, right], o[:8, right]], 0).astype(jnp.bfloat16)


def gather_blocks(y, groups, stage):
    quarters = y.shape[0] // groups
    rows = y.shape[1]
    lane = lax.broadcasted_iota(jnp.int32, (rows, LANES), 1) // 32
    odd, high = lane % 2 == 1, lane >= 2
    for g in range(groups):
        v = [y[g * quarters + t].astype(jnp.float32) for t in range(quarters)]
        w = [None] * 4
        for t in (0, 2):
            w[t] = jnp.where(odd, pltpu.roll(v[t + 1], 32, 1), v[t])
            w[t + 1] = jnp.where(odd, v[t + 1], pltpu.roll(v[t], LANES - 32, 1))
        u = [None] * 4
        for b in (0, 1):
            u[b] = jnp.where(high, pltpu.roll(w[b + 2], 64, 1), w[b])
            u[b + 2] = jnp.where(high, w[b + 2], pltpu.roll(w[b], 64, 1))
        for b in range(4):
            stage[b * rows : (b + 1) * rows, g * GRP : (g + 1) * GRP] = u[b].astype(jnp.bfloat16)


def owner_of(row, ways, core, far, flip, dz):
    x, y = lax.rem(row, 2), lax.rem(lax.div(row, 2), 2)
    dy = flip * (1 - core) + far * core
    dx = far * (1 - core) + flip * core
    x = x + dx - 2 * x * dx
    y = y + dy - 2 * y * dy
    return lax.rem(lax.div(row, 4) * 4 + 4 * dz, ways) + 2 * y + x


def products(row, core, lhs, near, far):
    ways = 2 * near.shape[0]
    for hop, blocks in enumerate((near, far)):
        for i in range(0, ways // 2, 2):
            both = jnp.dot(lhs, jnp.concatenate([blocks[i], blocks[i + 1]], 1), preferred_element_type=jnp.float32)
            for n in range(2):
                flip, dz = (i + n) // (ways // 4), (i + n) % (ways // 4)
                owner = owner_of(row, ways, core, hop, flip, dz)
                columns = pl.ds(pl.multiple_of(owner * LANES, LANES), LANES)
                yield columns, both[:, n * LANES : (n + 1) * LANES]


def first_kernel(place, y, hot, swap, near, far, total, mixed, stage):
    row, core = place[0], place[1]
    features = stage.shape[1]
    groups = features // GRP
    half = features // 2
    gather_blocks(y, groups, stage)
    rows = jnp.dot(hot[...], stage[...], preferred_element_type=jnp.float32).astype(jnp.bfloat16)
    for g in range(groups):
        part = slice(g * GRP, (g + 1) * GRP)
        mixed[:, part] = jnp.dot(rows[:, part], swap[...], preferred_element_type=jnp.float32).astype(jnp.bfloat16)
    own = mixed[:, pl.ds(pl.multiple_of(core * half, half), half)]
    for columns, block in products(row, core, own, near, far):
        total[:, columns] = block


def last_kernel(place, mixed, total, near, far, out, held, sems):
    row, core = place[0], 1 - place[1]
    half = mixed.shape[1] // 2
    other = mixed[:, pl.ds(pl.multiple_of(core * half, half), half)]
    copies = []
    for columns, block in products(row, core, other, near, far):
        held[:, columns] = (total[:, columns] + block).astype(jnp.bfloat16)
        copies.append(pltpu.make_async_copy(held.at[:, columns], out.at[:, columns], sems.at[len(copies)]))
        copies[-1].start()
    for copy in copies:
        copy.wait()


def vmem(count):
    return [pl.BlockSpec(memory_space=pltpu.VMEM)] * count


def shards(tokens, proj_in, proj_out):
    seq_rows = tokens[0]
    span, width = seq_rows.shape
    depth, features = proj_in.shape
    ways = lax.axis_size("row")
    groups = features // GRP
    quarters = ways // groups
    pairs = GRP // 2 // quarters
    bf16, f32 = jnp.bfloat16, jnp.float32
    room = pltpu.CompilerParams(vmem_limit_bytes=16 << 20)

    me = lax.axis_index("col")
    half = features // 2
    swap_cores = lambda v: lax.ppermute(v, "col", [(0, 1), (1, 0)])
    along = lambda v, to: lax.ppermute(v, ("row", "col"), [(2 * r + c, 2 * to(r, c) + c) for r in range(ways) for c in (0, 1)])
    other_w = swap_cores(proj_in)
    table = jnp.asarray(channel_table(quarters, pairs), bf16)
    hbm = pl.BlockSpec(memory_space=pltpu.MemorySpace.HBM)
    smem = pl.BlockSpec(memory_space=pltpu.SMEM)
    part, tok_other, table, mine = pl.pallas_call(
        own_kernel,
        in_specs=[smem] + [hbm] * 4,
        out_specs=vmem(4),
        out_shape=[
            jax.ShapeDtypeStruct((span, features), f32),
            jax.ShapeDtypeStruct((span, depth), bf16),
            jax.ShapeDtypeStruct(table.shape, bf16),
            jax.ShapeDtypeStruct((half, LANES), bf16),
        ],
        scratch_shapes=[
            pltpu.VMEM((span, depth), bf16),
            pltpu.VMEM((depth, features), bf16),
            pltpu.SemaphoreType.DMA((5,)),
        ],
        cost_estimate=pl.CostEstimate(flops=2 * span * depth * features, bytes_accessed=2 << 20, transcendentals=0),
        compiler_params=room,
        name="own_half",
    )(me[None], *[pltpu.with_memory_space_constraint(v, pltpu.MemorySpace.HBM) for v in (seq_rows, proj_in, table, proj_out)])
    ring = [mine]
    for dz in range(1, ways // 4):
        ring.append(along(mine, lambda r, c: (r - 4 * dz) % ways))
    sent = pl.pallas_call(
        send_kernel,
        in_specs=vmem(4),
        out_specs=vmem(1)[0],
        out_shape=jax.ShapeDtypeStruct((ways, 48, LANES), bf16),
        scratch_shapes=[pltpu.VMEM((2 * LANES, features), bf16)],
        cost_estimate=pl.CostEstimate(flops=2 * span * depth * features, bytes_accessed=2 << 20, transcendentals=0),
        compiler_params=room,
        name="send",
    )(tok_other, other_w, part, table)
    *ring, _ = lax.optimization_barrier((*ring, sent))
    ring = jnp.stack(ring, 0)
    plane = along(ring, lambda r, c: r ^ (1 if c else 2))
    held = lax.all_to_all(sent, "row", 0, 0, tiled=True)
    held, plane = lax.optimization_barrier((held, plane))
    near = jnp.concatenate([ring, plane], 0)
    far = along(near, lambda r, c: r ^ (2 if c else 1))
    near_other = swap_cores(near)

    even, odd = position_tables(ways, span)
    even, odd = jnp.asarray(even, bf16), jnp.asarray(odd, bf16)
    twist = jnp.asarray(twiddle_table(ways, span), f32)
    special = lax.rem(lax.axis_index("row"), quarters)[None]
    spectra = pl.pallas_call(
        mix_kernel,
        in_specs=[pl.BlockSpec(memory_space=pltpu.SMEM)] + vmem(4),
        out_specs=vmem(1)[0],
        out_shape=jax.ShapeDtypeStruct((ways, 48, LANES), bf16),
        scratch_shapes=[pltpu.VMEM((ways * 32, 4 * LANES), bf16)],
        compiler_params=room,
        name="mix",
    )(special, held, even, odd, twist)

    back = lax.all_to_all(spectra, "row", 0, 0, tiled=True)

    back, far = lax.optimization_barrier((back, far))
    far_other = swap_cores(far)
    hot = jnp.asarray(row_order(span), bf16)
    swap = np.zeros((GRP, GRP))
    swap[np.arange(GRP), channel_order(1, quarters, pairs)] = 1
    place = jnp.stack([lax.axis_index("row"), me])
    wide = ways * LANES
    total, mixed = pl.pallas_call(
        first_kernel,
        in_specs=[smem] + vmem(5),
        out_specs=vmem(2),
        out_shape=[jax.ShapeDtypeStruct((span, wide), f32), jax.ShapeDtypeStruct((span, features), bf16)],
        scratch_shapes=[pltpu.VMEM((span, features), bf16)],
        cost_estimate=pl.CostEstimate(flops=span * wide * features, bytes_accessed=2 << 20, transcendentals=0),
        compiler_params=room,
        name="first",
    )(place, back, hot, jnp.asarray(swap, bf16), near, far)
    result = pl.pallas_call(
        last_kernel,
        in_specs=[smem] + vmem(4),
        out_specs=hbm,
        out_shape=jax.ShapeDtypeStruct((span, wide), bf16),
        scratch_shapes=[pltpu.VMEM((span, wide), bf16), pltpu.SemaphoreType.DMA((ways,))],
        cost_estimate=pl.CostEstimate(flops=span * wide * features, bytes_accessed=2 << 20, transcendentals=0),
        compiler_params=room,
        name="last",
    )(place, mixed, total, near_other, far_other)
    return result[None]


def fits(mesh, tokens, proj_in, proj_out):
    ways, cols = mesh.shape["row"], mesh.shape["col"]
    features = proj_in.shape[1]
    span = tokens.shape[1] // ways
    return (
        features % GRP == 0
        and ways == 4 * (features // GRP) == 16
        and span == 12 * ways
        and cols == 2
        and tokens.shape[0] == cols
        and proj_out.shape[1] == ways * LANES
    )


def solution(mesh):
    in_specs = (P("col", "row", None), P("col", None), P(None, "row"))
    out_specs = P("col", "row", None)

    def run(tokens, proj_in, proj_out):
        body = shards if fits(mesh, tokens, proj_in, proj_out) else general_shards
        return jax.shard_map(body, mesh=mesh, in_specs=in_specs, out_specs=out_specs, check_vma=False)(
            tokens, proj_in, proj_out
        )

    return run
```

```python
import math

import jax
import jax.numpy as jnp
import numpy as np
from jax import lax
from jax.experimental import pallas as pl
from jax.experimental.pallas import tpu as pltpu
from jax.sharding import PartitionSpec as P

GRP = 128
LANES = 128
highest = lax.Precision.HIGHEST
span_inner = 128


def circle(height, breadth, period):
    product = lax.iota(jnp.int32, height)[:, None] * lax.iota(jnp.int32, breadth)[None, :] % period
    angle = product.astype(jnp.float32) * (2.0 * math.pi / period)
    return (jnp.cos(angle), jnp.sin(angle))


def positions(piece):
    real_in = piece[0, 0]
    imag_in = piece[1, 0]
    count, length = real_in.shape
    outer = length // span_inner
    real_in = real_in.reshape(count, outer, span_inner)
    imag_in = imag_in.reshape(count, outer, span_inner)
    cos_one, sin_one = circle(outer, outer, outer)
    first_re = jnp.einsum("ab,kbq->kaq", cos_one, real_in, precision=highest) - jnp.einsum(
        "ab,kbq->kaq", sin_one, imag_in, precision=highest
    )
    first_im = jnp.einsum("ab,kbq->kaq", sin_one, real_in, precision=highest) + jnp.einsum(
        "ab,kbq->kaq", cos_one, imag_in, precision=highest
    )
    twist_c, twist_s = circle(outer, span_inner, length)
    turned_re = first_re * twist_c - first_im * twist_s
    turned_im = first_re * twist_s + first_im * twist_c
    cos_two, sin_two = circle(span_inner, span_inner, span_inner)
    factor = 1.0 / math.sqrt(GRP * length)
    real_out = jnp.einsum("kaq,qb->kba", turned_re, cos_two, precision=highest) - jnp.einsum(
        "kaq,qb->kba", turned_im, sin_two, precision=highest
    )
    real_out = real_out.reshape(count, length) * factor
    return real_out[:, None, :]


def general_shards(tokens, proj_in, proj_out):
    seq_rows = tokens[0]
    local_len = seq_rows.shape[0]
    features = proj_in.shape[1]
    groups = features // GRP
    mapped = jnp.dot(
        seq_rows,
        lax.all_gather(proj_in, "col", axis=0, tiled=True),
        preferred_element_type=jnp.float32,
    ).astype(jnp.bfloat16)
    values = mapped.astype(jnp.float32).reshape(local_len, groups, GRP)
    cos_c, sin_c = circle(GRP, GRP, GRP)
    real_part = jnp.einsum("pgc,cs->gsp", values, cos_c, precision=highest)
    imag_part = jnp.einsum("pgc,cs->gsp", values, sin_c, precision=highest)
    ways = lax.axis_size("row")
    slots = groups * cos_c.shape[1]
    per_dev = slots // ways
    stacked = jnp.stack(
        [real_part.reshape(ways, per_dev, local_len), imag_part.reshape(ways, per_dev, local_len)],
        0,
    )
    spectra = positions(lax.all_to_all(stacked, "row", split_axis=1, concat_axis=3, tiled=True))
    outgoing = spectra.astype(jnp.bfloat16)
    back = lax.all_to_all(outgoing, "row", split_axis=2, concat_axis=0, tiled=True)
    mixed = back.reshape(features, local_len)
    result = lax.dot_general(
        mixed,
        lax.all_gather(proj_out, "row", axis=1, tiled=True),
        (((0,), (0,)), ((), ())),
        preferred_element_type=jnp.float32,
    )
    return result.astype(jnp.bfloat16)[None]


def channel_table(quarters, pairs):
    c = np.arange(GRP)
    rows = []
    for t in range(quarters):
        j = pairs * t + np.arange(pairs)
        angle = 2 * np.pi * (j[:, None] * c % GRP) / GRP
        sine = np.sin(angle)
        if t == 0:
            sine[0] = np.cos(np.pi * c)
        rows += [np.cos(angle), sine]
    return np.concatenate(rows, 0)


def channel_order(groups, quarters, pairs):
    order = []
    for g in range(groups):
        for t in range(quarters):
            j = pairs * t + np.arange(pairs)
            mirror = (GRP - j) % GRP
            if t == 0:
                mirror[0] = GRP // 2
            order += list(g * GRP + j) + list(g * GRP + mirror)
    return np.array(order)


def position_tables(ways, span):
    per = span // ways
    q = np.arange(span)
    low = min(LANES, span)
    even = np.zeros((ways, 16, 4 * LANES))
    odd = np.zeros((ways, 16, 4 * LANES))
    for owner in range(ways):
        for m in range(per):
            angle = 2 * np.pi * (q * (per * owner + m) % span) / span
            row = np.zeros(4 * LANES)
            row[:low] = np.cos(angle[:low])
            row[LANES : LANES + low] = np.sin(angle[:low])
            row[2 * LANES : 2 * LANES + span - low] = np.cos(angle[low:])
            row[3 * LANES : 3 * LANES + span - low] = np.sin(angle[low:])
            even[owner, m] = row
            odd[owner, m if m < 8 else m + 4] = row
    return even.reshape(-1, 4 * LANES), odd.reshape(-1, 4 * LANES)


def twiddle_table(ways, span):
    length = ways * span
    factor = 1.0 / math.sqrt(GRP * length)
    q = np.arange(2 * LANES)
    angle = 2 * np.pi * (np.arange(ways)[:, None] * q % length) / length
    cos, sin = np.cos(angle) * factor, np.sin(angle) * factor
    return np.stack([cos[:, :LANES], sin[:, :LANES], cos[:, LANES:], sin[:, LANES:]], 1)


def row_order(span):
    chunk = []
    chunk += [(0, m) for m in range(8)] + [(2, m) for m in range(8)]
    for a in range(4):
        chunk += [((0, 2, 1, 3)[a], 8 + m) for m in range(4)]
    chunk += [(1, m) for m in range(8)] + [(3, m) for m in range(8)]
    rows = len(chunk)
    hot = np.zeros((span, span))
    for b in range(4):
        for i, (a, m) in enumerate(chunk):
            hot[16 * m + 4 * a + b, b * rows + i] = 1
    return hot


def own_kernel(core, tok, w, table, w_out, part, tok_other, table_copy, mine, tok_own, w_own, sems):
    depth = w_own.shape[0]
    half = mine.shape[0]
    me = core[0]
    columns = lambda which: pl.ds(pl.multiple_of(which * depth, depth), depth)
    copies = [
        pltpu.make_async_copy(tok.at[:, columns(me)], tok_own, sems.at[0]),
        pltpu.make_async_copy(w, w_own, sems.at[1]),
        pltpu.make_async_copy(w_out.at[pl.ds(pl.multiple_of(me * half, half), half), :], mine, sems.at[2]),
        pltpu.make_async_copy(tok.at[:, columns(1 - me)], tok_other, sems.at[3]),
        pltpu.make_async_copy(table, table_copy, sems.at[4]),
    ]
    for copy in copies:
        copy.start()
    copies[0].wait()
    copies[1].wait()
    part[...] = jnp.dot(tok_own[...], w_own[...], preferred_element_type=jnp.float32)
    for copy in copies[2:]:
        copy.wait()


def send_kernel(tok, w, part, table, out, padded):
    span, features = part.shape
    mapped = part[...] + jnp.dot(tok[...], w[...], preferred_element_type=jnp.float32)
    padded[pl.ds(0, span), :] = mapped.astype(jnp.bfloat16)
    padded[pl.ds(span, 2 * LANES - span), :] = jnp.zeros((2 * LANES - span, features), jnp.bfloat16)
    groups = features // GRP
    quarters = out.shape[0] // groups
    for g in range(groups):
        turned = lax.dot_general(
            table[...],
            padded[:, g * GRP : (g + 1) * GRP],
            (((1,), (1,)), ((), ())),
            preferred_element_type=jnp.float32,
        )
        for t in range(quarters):
            cos = turned[32 * t : 32 * t + 16]
            sin = turned[32 * t + 16 : 32 * t + 32]
            high = cos[:, LANES:] + pltpu.roll(sin[:, LANES:], LANES // 2, 1)
            d = g * quarters + t
            out[d, 0:16, :] = cos[:, :LANES].astype(jnp.bfloat16)
            out[d, 16:32, :] = sin[:, :LANES].astype(jnp.bfloat16)
            out[d, 32:48, :] = high.astype(jnp.bfloat16)


def fft4(a, b, c, d):
    (ar, ai), (br, bi), (cr, ci), (dr, di) = a, b, c, d
    sr, si, tr, ti = ar + cr, ai + ci, ar - cr, ai - ci
    ur, ui, vr, vi = br + dr, bi + di, br - dr, bi - di
    return [(sr + ur, si + ui), (tr + vi, ti - vr), (sr - ur, si - ui), (tr - vi, ti + vr)]


def turn(v, n):
    re, im = v
    n %= 16
    if n == 0:
        return v
    if n == 4:
        return (im, -re)
    if n == 2:
        h = math.sqrt(0.5)
        return ((re + im) * h, (im - re) * h)
    if n == 6:
        h = math.sqrt(0.5)
        return ((im - re) * h, -(re + im) * h)
    c, s = math.cos(2 * math.pi * n / 16), math.sin(2 * math.pi * n / 16)
    return (re * c + im * s, im * c - re * s)


def fft16(v):
    inner = [fft4(v[a], v[a + 4], v[a + 8], v[a + 12]) for a in range(4)]
    out = [None] * 16
    for f in range(4):
        col = fft4(*[turn(inner[a][f], a * f) for a in range(4)])
        for e in range(4):
            out[f + 4 * e] = col[e]
    return out


def mix_kernel(special, x, even, odd, twist, out, turned):
    ways = x.shape[0]
    first = (lax.broadcasted_iota(jnp.int32, (16, LANES), 0) == 0) & (special[0] == 0)
    for part in range(2):
        v = []
        for r in range(ways):
            if part == 0:
                re = x[r, 0:16, :].astype(jnp.float32)
                im = -x[r, 16:32, :].astype(jnp.float32)
            else:
                re = x[r, 32:48, :].astype(jnp.float32)
                im = -pltpu.roll(re, LANES // 2, 1)
            v.append((re, im))
        spec = fft16(v)
        for k in range(ways):
            pr, pi = spec[k]
            qr, qi = spec[-k % ways]
            qi = -qi
            ur = jnp.where(first, (pr + qr) * 0.5, pr)
            ui = jnp.where(first, (pi + qi) * 0.5, pi)
            wr = jnp.where(first, (qi - pi) * 0.5, qr)
            wi = jnp.where(first, (pr - qr) * 0.5, qi)
            c = twist[k, 2 * part : 2 * part + 1, :]
            s = twist[k, 2 * part + 1 : 2 * part + 2, :]
            lo = slice(2 * part * LANES, (2 * part + 1) * LANES)
            hi = slice((2 * part + 1) * LANES, (2 * part + 2) * LANES)
            turned[32 * k : 32 * k + 16, lo] = (ur * c + ui * s).astype(jnp.bfloat16)
            turned[32 * k : 32 * k + 16, hi] = (ui * c - ur * s).astype(jnp.bfloat16)
            turned[32 * k + 16 : 32 * k + 32, lo] = (wr * c + wi * s).astype(jnp.bfloat16)
            turned[32 * k + 16 : 32 * k + 32, hi] = (wi * c - wr * s).astype(jnp.bfloat16)
    half = turned.shape[0] // 2
    nt = (((1,), (1,)), ((), ()))
    one = lax.dot_general(even[...], turned[:half, :], nt, preferred_element_type=jnp.float32)
    two = lax.dot_general(odd[...], turned[half:, :], nt, preferred_element_type=jnp.float32)
    for r in range(ways):
        e, o = one[16 * r : 16 * r + 16], two[16 * r : 16 * r + 16]
        tail = e[8:] + o[8:]
        left, right = slice(0, LANES), slice(LANES, 2 * LANES)
        out[r, 0:16, :] = jnp.concatenate([e[:8, left], o[:8, left]], 0).astype(jnp.bfloat16)
        out[r, 16:32, :] = jnp.concatenate([tail[:, left], tail[:, right]], 0).astype(jnp.bfloat16)
        out[r, 32:48, :] = jnp.concatenate([e[:8, right], o[:8, right]], 0).astype(jnp.bfloat16)


def gather_blocks(y, groups, stage):
    quarters = y.shape[0] // groups
    rows = y.shape[1]
    lane = lax.broadcasted_iota(jnp.int32, (rows, LANES), 1) // 32
    odd, high = lane % 2 == 1, lane >= 2
    for g in range(groups):
        v = [y[g * quarters + t].astype(jnp.float32) for t in range(quarters)]
        w = [None] * 4
        for t in (0, 2):
            w[t] = jnp.where(odd, pltpu.roll(v[t + 1], 32, 1), v[t])
            w[t + 1] = jnp.where(odd, v[t + 1], pltpu.roll(v[t], LANES - 32, 1))
        u = [None] * 4
        for b in (0, 1):
            u[b] = jnp.where(high, pltpu.roll(w[b + 2], 64, 1), w[b])
            u[b + 2] = jnp.where(high, w[b + 2], pltpu.roll(w[b], 64, 1))
        for b in range(4):
            stage[b * rows : (b + 1) * rows, g * GRP : (g + 1) * GRP] = u[b].astype(jnp.bfloat16)


def owner_of(row, ways, core, far, flip, dz):
    x, y = lax.rem(row, 2), lax.rem(lax.div(row, 2), 2)
    dy = flip * (1 - core) + far * core
    dx = far * (1 - core) + flip * core
    x = x + dx - 2 * x * dx
    y = y + dy - 2 * y * dy
    return lax.rem(lax.div(row, 4) * 4 + 4 * dz, ways) + 2 * y + x


def products(row, core, lhs, near, far):
    ways = 2 * near.shape[0]
    for hop, blocks in enumerate((near, far)):
        for i in range(0, ways // 2, 2):
            both = jnp.dot(lhs, jnp.concatenate([blocks[i], blocks[i + 1]], 1), preferred_element_type=jnp.float32)
            for n in range(2):
                flip, dz = (i + n) // (ways // 4), (i + n) % (ways // 4)
                owner = owner_of(row, ways, core, hop, flip, dz)
                columns = pl.ds(pl.multiple_of(owner * LANES, LANES), LANES)
                yield columns, both[:, n * LANES : (n + 1) * LANES]


def first_kernel(place, y, hot, swap, near, far, total, mixed, stage):
    row, core = place[0], place[1]
    features = stage.shape[1]
    groups = features // GRP
    half = features // 2
    gather_blocks(y, groups, stage)
    rows = jnp.dot(hot[...], stage[...], preferred_element_type=jnp.float32).astype(jnp.bfloat16)
    for g in range(groups):
        part = slice(g * GRP, (g + 1) * GRP)
        mixed[:, part] = jnp.dot(rows[:, part], swap[...], preferred_element_type=jnp.float32).astype(jnp.bfloat16)
    own = mixed[:, pl.ds(pl.multiple_of(core * half, half), half)]
    for columns, block in products(row, core, own, near, far):
        total[:, columns] = block


def last_kernel(place, mixed, total, near, far, out, held, sems):
    row, core = place[0], 1 - place[1]
    half = mixed.shape[1] // 2
    other = mixed[:, pl.ds(pl.multiple_of(core * half, half), half)]
    copies = []
    for columns, block in products(row, core, other, near, far):
        held[:, columns] = (total[:, columns] + block).astype(jnp.bfloat16)
        copies.append(pltpu.make_async_copy(held.at[:, columns], out.at[:, columns], sems.at[len(copies)]))
        copies[-1].start()
    for copy in copies:
        copy.wait()


def vmem(count):
    return [pl.BlockSpec(memory_space=pltpu.VMEM)] * count


def shards(tokens, proj_in, proj_out):
    seq_rows = tokens[0]
    span, width = seq_rows.shape
    depth, features = proj_in.shape
    ways = lax.axis_size("row")
    groups = features // GRP
    quarters = ways // groups
    pairs = GRP // 2 // quarters
    bf16, f32 = jnp.bfloat16, jnp.float32
    room = pltpu.CompilerParams(vmem_limit_bytes=16 << 20)

    me = lax.axis_index("col")
    half = features // 2
    swap_cores = lambda v: lax.ppermute(v, "col", [(0, 1), (1, 0)])
    along = lambda v, to: lax.ppermute(v, ("row", "col"), [(2 * r + c, 2 * to(r, c) + c) for r in range(ways) for c in (0, 1)])
    other_w = swap_cores(proj_in)
    table = jnp.asarray(channel_table(quarters, pairs), bf16)
    hbm = pl.BlockSpec(memory_space=pltpu.MemorySpace.HBM)
    smem = pl.BlockSpec(memory_space=pltpu.SMEM)
    part, tok_other, table, mine = pl.pallas_call(
        own_kernel,
        in_specs=[smem] + [hbm] * 4,
        out_specs=vmem(4),
        out_shape=[
            jax.ShapeDtypeStruct((span, features), f32),
            jax.ShapeDtypeStruct((span, depth), bf16),
            jax.ShapeDtypeStruct(table.shape, bf16),
            jax.ShapeDtypeStruct((half, LANES), bf16),
        ],
        scratch_shapes=[
            pltpu.VMEM((span, depth), bf16),
            pltpu.VMEM((depth, features), bf16),
            pltpu.SemaphoreType.DMA((5,)),
        ],
        cost_estimate=pl.CostEstimate(flops=2 * span * depth * features, bytes_accessed=2 << 20, transcendentals=0),
        compiler_params=room,
        name="own_half",
    )(me[None], *[pltpu.with_memory_space_constraint(v, pltpu.MemorySpace.HBM) for v in (seq_rows, proj_in, table, proj_out)])
    ring = [mine]
    for dz in range(1, ways // 4):
        ring.append(along(mine, lambda r, c: (r - 4 * dz) % ways))
    sent = pl.pallas_call(
        send_kernel,
        in_specs=vmem(4),
        out_specs=vmem(1)[0],
        out_shape=jax.ShapeDtypeStruct((ways, 48, LANES), bf16),
        scratch_shapes=[pltpu.VMEM((2 * LANES, features), bf16)],
        cost_estimate=pl.CostEstimate(flops=2 * span * depth * features, bytes_accessed=2 << 20, transcendentals=0),
        compiler_params=room,
        name="send",
    )(tok_other, other_w, part, table)
    *ring, _ = lax.optimization_barrier((*ring, sent))
    ring = jnp.stack(ring, 0)
    plane = along(ring, lambda r, c: r ^ (1 if c else 2))
    held = lax.all_to_all(sent, "row", 0, 0, tiled=True)

    even, odd = position_tables(ways, span)
    even, odd = jnp.asarray(even, bf16), jnp.asarray(odd, bf16)
    twist = jnp.asarray(twiddle_table(ways, span), f32)
    special = lax.rem(lax.axis_index("row"), quarters)[None]
    spectra = pl.pallas_call(
        mix_kernel,
        in_specs=[pl.BlockSpec(memory_space=pltpu.SMEM)] + vmem(4),
        out_specs=vmem(1)[0],
        out_shape=jax.ShapeDtypeStruct((ways, 48, LANES), bf16),
        scratch_shapes=[pltpu.VMEM((ways * 32, 4 * LANES), bf16)],
        compiler_params=room,
        name="mix",
    )(special, held, even, odd, twist)

    spectra, plane = lax.optimization_barrier((spectra, plane))
    near = jnp.concatenate([ring, plane], 0)
    far = along(near, lambda r, c: r ^ (2 if c else 1))
    near_other = swap_cores(near)
    back = lax.all_to_all(spectra, "row", 0, 0, tiled=True)

    back, far = lax.optimization_barrier((back, far))
    far_other = swap_cores(far)
    hot = jnp.asarray(row_order(span), bf16)
    swap = np.zeros((GRP, GRP))
    swap[np.arange(GRP), channel_order(1, quarters, pairs)] = 1
    place = jnp.stack([lax.axis_index("row"), me])
    wide = ways * LANES
    total, mixed = pl.pallas_call(
        first_kernel,
        in_specs=[smem] + vmem(5),
        out_specs=vmem(2),
        out_shape=[jax.ShapeDtypeStruct((span, wide), f32), jax.ShapeDtypeStruct((span, features), bf16)],
        scratch_shapes=[pltpu.VMEM((span, features), bf16)],
        cost_estimate=pl.CostEstimate(flops=span * wide * features, bytes_accessed=2 << 20, transcendentals=0),
        compiler_params=room,
        name="first",
    )(place, back, hot, jnp.asarray(swap, bf16), near, far)
    result = pl.pallas_call(
        last_kernel,
        in_specs=[smem] + vmem(4),
        out_specs=hbm,
        out_shape=jax.ShapeDtypeStruct((span, wide), bf16),
        scratch_shapes=[pltpu.VMEM((span, wide), bf16), pltpu.SemaphoreType.DMA((ways,))],
        cost_estimate=pl.CostEstimate(flops=span * wide * features, bytes_accessed=2 << 20, transcendentals=0),
        compiler_params=room,
        name="last",
    )(place, mixed, total, near_other, far_other)
    return result[None]


def fits(mesh, tokens, proj_in, proj_out):
    ways, cols = mesh.shape["row"], mesh.shape["col"]
    features = proj_in.shape[1]
    span = tokens.shape[1] // ways
    return (
        features % GRP == 0
        and ways == 4 * (features // GRP) == 16
        and span == 12 * ways
        and cols == 2
        and tokens.shape[0] == cols
        and proj_out.shape[1] == ways * LANES
    )


def solution(mesh):
    in_specs = (P("col", "row", None), P("col", None), P(None, "row"))
    out_specs = P("col", "row", None)

    def run(tokens, proj_in, proj_out):
        body = shards if fits(mesh, tokens, proj_in, proj_out) else general_shards
        return jax.shard_map(body, mesh=mesh, in_specs=in_specs, out_specs=out_specs, check_vma=False)(
            tokens, proj_in, proj_out
        )

    return run
```

```python
import math

import jax
import jax.numpy as jnp
import numpy as np
from jax import lax
from jax.experimental import pallas as pl
from jax.experimental.pallas import tpu as pltpu
from jax.sharding import PartitionSpec as P

GRP = 128
LANES = 128
highest = lax.Precision.HIGHEST
span_inner = 128


def circle(height, breadth, period):
    product = lax.iota(jnp.int32, height)[:, None] * lax.iota(jnp.int32, breadth)[None, :] % period
    angle = product.astype(jnp.float32) * (2.0 * math.pi / period)
    return (jnp.cos(angle), jnp.sin(angle))


def positions(piece):
    real_in = piece[0, 0]
    imag_in = piece[1, 0]
    count, length = real_in.shape
    outer = length // span_inner
    real_in = real_in.reshape(count, outer, span_inner)
    imag_in = imag_in.reshape(count, outer, span_inner)
    cos_one, sin_one = circle(outer, outer, outer)
    first_re = jnp.einsum("ab,kbq->kaq", cos_one, real_in, precision=highest) - jnp.einsum(
        "ab,kbq->kaq", sin_one, imag_in, precision=highest
    )
    first_im = jnp.einsum("ab,kbq->kaq", sin_one, real_in, precision=highest) + jnp.einsum(
        "ab,kbq->kaq", cos_one, imag_in, precision=highest
    )
    twist_c, twist_s = circle(outer, span_inner, length)
    turned_re = first_re * twist_c - first_im * twist_s
    turned_im = first_re * twist_s + first_im * twist_c
    cos_two, sin_two = circle(span_inner, span_inner, span_inner)
    factor = 1.0 / math.sqrt(GRP * length)
    real_out = jnp.einsum("kaq,qb->kba", turned_re, cos_two, precision=highest) - jnp.einsum(
        "kaq,qb->kba", turned_im, sin_two, precision=highest
    )
    real_out = real_out.reshape(count, length) * factor
    return real_out[:, None, :]


def general_shards(tokens, proj_in, proj_out):
    seq_rows = tokens[0]
    local_len = seq_rows.shape[0]
    features = proj_in.shape[1]
    groups = features // GRP
    mapped = jnp.dot(
        seq_rows,
        lax.all_gather(proj_in, "col", axis=0, tiled=True),
        preferred_element_type=jnp.float32,
    ).astype(jnp.bfloat16)
    values = mapped.astype(jnp.float32).reshape(local_len, groups, GRP)
    cos_c, sin_c = circle(GRP, GRP, GRP)
    real_part = jnp.einsum("pgc,cs->gsp", values, cos_c, precision=highest)
    imag_part = jnp.einsum("pgc,cs->gsp", values, sin_c, precision=highest)
    ways = lax.axis_size("row")
    slots = groups * cos_c.shape[1]
    per_dev = slots // ways
    stacked = jnp.stack(
        [real_part.reshape(ways, per_dev, local_len), imag_part.reshape(ways, per_dev, local_len)],
        0,
    )
    spectra = positions(lax.all_to_all(stacked, "row", split_axis=1, concat_axis=3, tiled=True))
    outgoing = spectra.astype(jnp.bfloat16)
    back = lax.all_to_all(outgoing, "row", split_axis=2, concat_axis=0, tiled=True)
    mixed = back.reshape(features, local_len)
    result = lax.dot_general(
        mixed,
        lax.all_gather(proj_out, "row", axis=1, tiled=True),
        (((0,), (0,)), ((), ())),
        preferred_element_type=jnp.float32,
    )
    return result.astype(jnp.bfloat16)[None]


def channel_table(quarters, pairs):
    c = np.arange(GRP)
    rows = []
    for t in range(quarters):
        j = pairs * t + np.arange(pairs)
        angle = 2 * np.pi * (j[:, None] * c % GRP) / GRP
        sine = np.sin(angle)
        if t == 0:
            sine[0] = np.cos(np.pi * c)
        rows += [np.cos(angle), sine]
    return np.concatenate(rows, 0)


def channel_order(groups, quarters, pairs):
    order = []
    for g in range(groups):
        for t in range(quarters):
            j = pairs * t + np.arange(pairs)
            mirror = (GRP - j) % GRP
            if t == 0:
                mirror[0] = GRP // 2
            order += list(g * GRP + j) + list(g * GRP + mirror)
    return np.array(order)


def position_tables(ways, span):
    per = span // ways
    q = np.arange(span)
    low = min(LANES, span)
    even = np.zeros((ways, 16, 4 * LANES))
    odd = np.zeros((ways, 16, 4 * LANES))
    for owner in range(ways):
        for m in range(per):
            angle = 2 * np.pi * (q * (per * owner + m) % span) / span
            row = np.zeros(4 * LANES)
            row[:low] = np.cos(angle[:low])
            row[LANES : LANES + low] = np.sin(angle[:low])
            row[2 * LANES : 2 * LANES + span - low] = np.cos(angle[low:])
            row[3 * LANES : 3 * LANES + span - low] = np.sin(angle[low:])
            even[owner, m] = row
            odd[owner, m if m < 8 else m + 4] = row
    return even.reshape(-1, 4 * LANES), odd.reshape(-1, 4 * LANES)


def twiddle_table(ways, span):
    length = ways * span
    factor = 1.0 / math.sqrt(GRP * length)
    q = np.arange(2 * LANES)
    angle = 2 * np.pi * (np.arange(ways)[:, None] * q % length) / length
    cos, sin = np.cos(angle) * factor, np.sin(angle) * factor
    return np.stack([cos[:, :LANES], sin[:, :LANES], cos[:, LANES:], sin[:, LANES:]], 1)


def row_order(span):
    chunk = []
    chunk += [(0, m) for m in range(8)] + [(2, m) for m in range(8)]
    for a in range(4):
        chunk += [((0, 2, 1, 3)[a], 8 + m) for m in range(4)]
    chunk += [(1, m) for m in range(8)] + [(3, m) for m in range(8)]
    rows = len(chunk)
    hot = np.zeros((span, span))
    for b in range(4):
        for i, (a, m) in enumerate(chunk):
            hot[16 * m + 4 * a + b, b * rows + i] = 1
    return hot


def fetch_kernel(core, w_out, tok, w, table, mine, tok_copy, w_copy, table_copy, sems):
    half = mine.shape[0]
    rows = pl.ds(pl.multiple_of(core[0] * half, half), half)
    copies = [
        pltpu.make_async_copy(w_out.at[rows, :], mine, sems.at[0]),
        pltpu.make_async_copy(tok, tok_copy, sems.at[1]),
        pltpu.make_async_copy(w, w_copy, sems.at[2]),
        pltpu.make_async_copy(table, table_copy, sems.at[3]),
    ]
    for copy in copies:
        copy.start()
    for copy in copies:
        copy.wait()


def send_kernel(core, tok, w_own, w_other, table, out, padded):
    span, features = tok.shape[0], w_own.shape[1]
    depth = w_own.shape[0]
    columns = lambda which: pl.ds(pl.multiple_of(which * depth, depth), depth)
    mapped = jnp.dot(tok[:, columns(core[0])], w_own[...], preferred_element_type=jnp.float32) + jnp.dot(
        tok[:, columns(1 - core[0])], w_other[...], preferred_element_type=jnp.float32
    )
    padded[pl.ds(0, span), :] = mapped.astype(jnp.bfloat16)
    padded[pl.ds(span, 2 * LANES - span), :] = jnp.zeros((2 * LANES - span, features), jnp.bfloat16)
    groups = features // GRP
    quarters = out.shape[0] // groups
    for g in range(groups):
        turned = lax.dot_general(
            table[...],
            padded[:, g * GRP : (g + 1) * GRP],
            (((1,), (1,)), ((), ())),
            preferred_element_type=jnp.float32,
        )
        for t in range(quarters):
            cos = turned[32 * t : 32 * t + 16]
            sin = turned[32 * t + 16 : 32 * t + 32]
            high = cos[:, LANES:] + pltpu.roll(sin[:, LANES:], LANES // 2, 1)
            d = g * quarters + t
            out[d, 0:16, :] = cos[:, :LANES].astype(jnp.bfloat16)
            out[d, 16:32, :] = sin[:, :LANES].astype(jnp.bfloat16)
            out[d, 32:48, :] = high.astype(jnp.bfloat16)


def fft4(a, b, c, d):
    (ar, ai), (br, bi), (cr, ci), (dr, di) = a, b, c, d
    sr, si, tr, ti = ar + cr, ai + ci, ar - cr, ai - ci
    ur, ui, vr, vi = br + dr, bi + di, br - dr, bi - di
    return [(sr + ur, si + ui), (tr + vi, ti - vr), (sr - ur, si - ui), (tr - vi, ti + vr)]


def turn(v, n):
    re, im = v
    n %= 16
    if n == 0:
        return v
    if n == 4:
        return (im, -re)
    if n == 2:
        h = math.sqrt(0.5)
        return ((re + im) * h, (im - re) * h)
    if n == 6:
        h = math.sqrt(0.5)
        return ((im - re) * h, -(re + im) * h)
    c, s = math.cos(2 * math.pi * n / 16), math.sin(2 * math.pi * n / 16)
    return (re * c + im * s, im * c - re * s)


def fft16(v):
    inner = [fft4(v[a], v[a + 4], v[a + 8], v[a + 12]) for a in range(4)]
    out = [None] * 16
    for f in range(4):
        col = fft4(*[turn(inner[a][f], a * f) for a in range(4)])
        for e in range(4):
            out[f + 4 * e] = col[e]
    return out


def mix_kernel(special, x, even, odd, twist, out, turned):
    ways = x.shape[0]
    first = (lax.broadcasted_iota(jnp.int32, (16, LANES), 0) == 0) & (special[0] == 0)
    for part in range(2):
        v = []
        for r in range(ways):
            if part == 0:
                re = x[r, 0:16, :].astype(jnp.float32)
                im = -x[r, 16:32, :].astype(jnp.float32)
            else:
                re = x[r, 32:48, :].astype(jnp.float32)
                im = -pltpu.roll(re, LANES // 2, 1)
            v.append((re, im))
        spec = fft16(v)
        for k in range(ways):
            pr, pi = spec[k]
            qr, qi = spec[-k % ways]
            qi = -qi
            ur = jnp.where(first, (pr + qr) * 0.5, pr)
            ui = jnp.where(first, (pi + qi) * 0.5, pi)
            wr = jnp.where(first, (qi - pi) * 0.5, qr)
            wi = jnp.where(first, (pr - qr) * 0.5, qi)
            c = twist[k, 2 * part : 2 * part + 1, :]
            s = twist[k, 2 * part + 1 : 2 * part + 2, :]
            lo = slice(2 * part * LANES, (2 * part + 1) * LANES)
            hi = slice((2 * part + 1) * LANES, (2 * part + 2) * LANES)
            turned[32 * k : 32 * k + 16, lo] = (ur * c + ui * s).astype(jnp.bfloat16)
            turned[32 * k : 32 * k + 16, hi] = (ui * c - ur * s).astype(jnp.bfloat16)
            turned[32 * k + 16 : 32 * k + 32, lo] = (wr * c + wi * s).astype(jnp.bfloat16)
            turned[32 * k + 16 : 32 * k + 32, hi] = (wi * c - wr * s).astype(jnp.bfloat16)
    half = turned.shape[0] // 2
    nt = (((1,), (1,)), ((), ()))
    one = lax.dot_general(even[...], turned[:half, :], nt, preferred_element_type=jnp.float32)
    two = lax.dot_general(odd[...], turned[half:, :], nt, preferred_element_type=jnp.float32)
    for r in range(ways):
        e, o = one[16 * r : 16 * r + 16], two[16 * r : 16 * r + 16]
        tail = e[8:] + o[8:]
        left, right = slice(0, LANES), slice(LANES, 2 * LANES)
        out[r, 0:16, :] = jnp.concatenate([e[:8, left], o[:8, left]], 0).astype(jnp.bfloat16)
        out[r, 16:32, :] = jnp.concatenate([tail[:, left], tail[:, right]], 0).astype(jnp.bfloat16)
        out[r, 32:48, :] = jnp.concatenate([e[:8, right], o[:8, right]], 0).astype(jnp.bfloat16)


def gather_blocks(y, groups, stage):
    quarters = y.shape[0] // groups
    rows = y.shape[1]
    lane = lax.broadcasted_iota(jnp.int32, (rows, LANES), 1) // 32
    odd, high = lane % 2 == 1, lane >= 2
    for g in range(groups):
        v = [y[g * quarters + t].astype(jnp.float32) for t in range(quarters)]
        w = [None] * 4
        for t in (0, 2):
            w[t] = jnp.where(odd, pltpu.roll(v[t + 1], 32, 1), v[t])
            w[t + 1] = jnp.where(odd, v[t + 1], pltpu.roll(v[t], LANES - 32, 1))
        u = [None] * 4
        for b in (0, 1):
            u[b] = jnp.where(high, pltpu.roll(w[b + 2], 64, 1), w[b])
            u[b + 2] = jnp.where(high, w[b + 2], pltpu.roll(w[b], 64, 1))
        for b in range(4):
            stage[b * rows : (b + 1) * rows, g * GRP : (g + 1) * GRP] = u[b].astype(jnp.bfloat16)


def owner_of(row, ways, core, far, flip, dz):
    x, y = lax.rem(row, 2), lax.rem(lax.div(row, 2), 2)
    dy = flip * (1 - core) + far * core
    dx = far * (1 - core) + flip * core
    x = x + dx - 2 * x * dx
    y = y + dy - 2 * y * dy
    return lax.rem(lax.div(row, 4) * 4 + 4 * dz, ways) + 2 * y + x


def products(row, core, lhs, near, far):
    ways = 2 * (far if near is None else near).shape[0]
    for hop, blocks in enumerate((near, far)):
        if blocks is None:
            continue
        for i in range(0, ways // 2, 2):
            both = jnp.dot(lhs, jnp.concatenate([blocks[i], blocks[i + 1]], 1), preferred_element_type=jnp.float32)
            for n in range(2):
                flip, dz = (i + n) // (ways // 4), (i + n) % (ways // 4)
                owner = owner_of(row, ways, core, hop, flip, dz)
                columns = pl.ds(pl.multiple_of(owner * LANES, LANES), LANES)
                yield columns, both[:, n * LANES : (n + 1) * LANES]


def first_kernel(place, y, hot, swap, near, far, near_other, total, mixed, stage):
    row, core = place[0], place[1]
    features = stage.shape[1]
    groups = features // GRP
    half = features // 2
    gather_blocks(y, groups, stage)
    rows = jnp.dot(hot[...], stage[...], preferred_element_type=jnp.float32).astype(jnp.bfloat16)
    for g in range(groups):
        part = slice(g * GRP, (g + 1) * GRP)
        mixed[:, part] = jnp.dot(rows[:, part], swap[...], preferred_element_type=jnp.float32).astype(jnp.bfloat16)
    own = mixed[:, pl.ds(pl.multiple_of(core * half, half), half)]
    for columns, block in products(row, core, own, near, far):
        total[:, columns] = block
    other = mixed[:, pl.ds(pl.multiple_of((1 - core) * half, half), half)]
    for columns, block in products(row, 1 - core, other, near_other, None):
        total[:, columns] += block


def last_kernel(place, mixed, total, far, out, held, sems):
    row, core = place[0], 1 - place[1]
    half = mixed.shape[1] // 2
    other = mixed[:, pl.ds(pl.multiple_of(core * half, half), half)]
    copies = []

    def finish(columns, block):
        held[:, columns] = block.astype(jnp.bfloat16)
        copies.append(pltpu.make_async_copy(held.at[:, columns], out.at[:, columns], sems.at[len(copies)]))
        copies[-1].start()

    ways = 2 * far.shape[0]
    for i in range(ways // 2):
        flip, dz = i // (ways // 4), i % (ways // 4)
        owner = owner_of(row, ways, core, 0, flip, dz)
        columns = pl.ds(pl.multiple_of(owner * LANES, LANES), LANES)
        finish(columns, total[:, columns])
    for columns, block in products(row, core, other, None, far):
        finish(columns, total[:, columns] + block)
    for copy in copies:
        copy.wait()


def vmem(count):
    return [pl.BlockSpec(memory_space=pltpu.VMEM)] * count


def shards(tokens, proj_in, proj_out):
    seq_rows = tokens[0]
    span, width = seq_rows.shape
    depth, features = proj_in.shape
    ways = lax.axis_size("row")
    groups = features // GRP
    quarters = ways // groups
    pairs = GRP // 2 // quarters
    bf16, f32 = jnp.bfloat16, jnp.float32
    room = pltpu.CompilerParams(vmem_limit_bytes=16 << 20)

    me = lax.axis_index("col")
    half = features // 2
    swap_cores = lambda v: lax.ppermute(v, "col", [(0, 1), (1, 0)])
    along = lambda v, to: lax.ppermute(v, ("row", "col"), [(2 * r + c, 2 * to(r, c) + c) for r in range(ways) for c in (0, 1)])
    other_w = swap_cores(proj_in)
    table = jnp.asarray(channel_table(quarters, pairs), bf16)
    hbm = pl.BlockSpec(memory_space=pltpu.MemorySpace.HBM)
    smem = pl.BlockSpec(memory_space=pltpu.SMEM)
    mine, tok, w_own, table = pl.pallas_call(
        fetch_kernel,
        in_specs=[smem] + [hbm] * 4,
        out_specs=vmem(4),
        out_shape=[
            jax.ShapeDtypeStruct((half, LANES), bf16),
            jax.ShapeDtypeStruct(seq_rows.shape, bf16),
            jax.ShapeDtypeStruct(proj_in.shape, bf16),
            jax.ShapeDtypeStruct(table.shape, bf16),
        ],
        scratch_shapes=[pltpu.SemaphoreType.DMA((4,))],
        compiler_params=room,
        name="fetch",
    )(me[None], *[pltpu.with_memory_space_constraint(v, pltpu.MemorySpace.HBM) for v in (proj_out, seq_rows, proj_in, table)])
    ring = [mine]
    for dz in range(1, ways // 4):
        ring.append(along(mine, lambda r, c: (r - 4 * dz) % ways))
    sent = pl.pallas_call(
        send_kernel,
        in_specs=[smem] + vmem(4),
        out_specs=vmem(1)[0],
        out_shape=jax.ShapeDtypeStruct((ways, 48, LANES), bf16),
        scratch_shapes=[pltpu.VMEM((2 * LANES, features), bf16)],
        cost_estimate=pl.CostEstimate(flops=2 * span * depth * features, bytes_accessed=2 << 20, transcendentals=0),
        compiler_params=room,
        name="send",
    )(me[None], tok, w_own, other_w, table)
    *ring, _ = lax.optimization_barrier((*ring, sent))
    ring = jnp.stack(ring, 0)
    plane = along(ring, lambda r, c: r ^ (1 if c else 2))
    held = lax.all_to_all(sent, "row", 0, 0, tiled=True)

    even, odd = position_tables(ways, span)
    even, odd = jnp.asarray(even, bf16), jnp.asarray(odd, bf16)
    twist = jnp.asarray(twiddle_table(ways, span), f32)
    special = lax.rem(lax.axis_index("row"), quarters)[None]
    spectra = pl.pallas_call(
        mix_kernel,
        in_specs=[pl.BlockSpec(memory_space=pltpu.SMEM)] + vmem(4),
        out_specs=vmem(1)[0],
        out_shape=jax.ShapeDtypeStruct((ways, 48, LANES), bf16),
        scratch_shapes=[pltpu.VMEM((ways * 32, 4 * LANES), bf16)],
        compiler_params=room,
        name="mix",
    )(special, held, even, odd, twist)

    spectra, plane = lax.optimization_barrier((spectra, plane))
    near = jnp.concatenate([ring, plane], 0)
    far = along(near, lambda r, c: r ^ (2 if c else 1))
    near_other = swap_cores(near)
    back = lax.all_to_all(spectra, "row", 0, 0, tiled=True)

    back, far = lax.optimization_barrier((back, far))
    far_other = swap_cores(far)
    hot = jnp.asarray(row_order(span), bf16)
    swap = np.zeros((GRP, GRP))
    swap[np.arange(GRP), channel_order(1, quarters, pairs)] = 1
    place = jnp.stack([lax.axis_index("row"), me])
    wide = ways * LANES
    total, mixed = pl.pallas_call(
        first_kernel,
        in_specs=[smem] + vmem(6),
        out_specs=vmem(2),
        out_shape=[jax.ShapeDtypeStruct((span, wide), f32), jax.ShapeDtypeStruct((span, features), bf16)],
        scratch_shapes=[pltpu.VMEM((span, features), bf16)],
        cost_estimate=pl.CostEstimate(flops=span * wide * features, bytes_accessed=2 << 20, transcendentals=0),
        compiler_params=room,
        name="first",
    )(place, back, hot, jnp.asarray(swap, bf16), near, far, near_other)
    result = pl.pallas_call(
        last_kernel,
        in_specs=[smem] + vmem(3),
        out_specs=hbm,
        out_shape=jax.ShapeDtypeStruct((span, wide), bf16),
        scratch_shapes=[pltpu.VMEM((span, wide), bf16), pltpu.SemaphoreType.DMA((ways,))],
        cost_estimate=pl.CostEstimate(flops=span * wide * features, bytes_accessed=2 << 20, transcendentals=0),
        compiler_params=room,
        name="last",
    )(place, mixed, total, far_other)
    return result[None]


def fits(mesh, tokens, proj_in, proj_out):
    ways, cols = mesh.shape["row"], mesh.shape["col"]
    features = proj_in.shape[1]
    span = tokens.shape[1] // ways
    return (
        features % GRP == 0
        and ways == 4 * (features // GRP) == 16
        and span == 12 * ways
        and cols == 2
        and tokens.shape[0] == cols
        and proj_out.shape[1] == ways * LANES
    )


def solution(mesh):
    in_specs = (P("col", "row", None), P("col", None), P(None, "row"))
    out_specs = P("col", "row", None)

    def run(tokens, proj_in, proj_out):
        body = shards if fits(mesh, tokens, proj_in, proj_out) else general_shards
        return jax.shard_map(body, mesh=mesh, in_specs=in_specs, out_specs=out_specs, check_vma=False)(
            tokens, proj_in, proj_out
        )

    return run
```

```python
import math

import jax
import jax.numpy as jnp
import numpy as np
from jax import lax
from jax.experimental import pallas as pl
from jax.experimental.pallas import tpu as pltpu
from jax.sharding import PartitionSpec as P


GRP = 128
LANES = 128
highest = lax.Precision.HIGHEST
span_inner = 128


def circle(height, breadth, period):
    product = lax.iota(jnp.int32, height)[:, None] * lax.iota(jnp.int32, breadth)[None, :] % period
    angle = product.astype(jnp.float32) * (2.0 * math.pi / period)
    return (jnp.cos(angle), jnp.sin(angle))


def positions(piece):
    real_in = piece[0, 0]
    imag_in = piece[1, 0]
    count, length = real_in.shape
    outer = length // span_inner
    real_in = real_in.reshape(count, outer, span_inner)
    imag_in = imag_in.reshape(count, outer, span_inner)
    cos_one, sin_one = circle(outer, outer, outer)
    first_re = jnp.einsum("ab,kbq->kaq", cos_one, real_in, precision=highest) - jnp.einsum(
        "ab,kbq->kaq", sin_one, imag_in, precision=highest
    )
    first_im = jnp.einsum("ab,kbq->kaq", sin_one, real_in, precision=highest) + jnp.einsum(
        "ab,kbq->kaq", cos_one, imag_in, precision=highest
    )
    twist_c, twist_s = circle(outer, span_inner, length)
    turned_re = first_re * twist_c - first_im * twist_s
    turned_im = first_re * twist_s + first_im * twist_c
    cos_two, sin_two = circle(span_inner, span_inner, span_inner)
    factor = 1.0 / math.sqrt(GRP * length)
    real_out = jnp.einsum("kaq,qb->kba", turned_re, cos_two, precision=highest) - jnp.einsum(
        "kaq,qb->kba", turned_im, sin_two, precision=highest
    )
    real_out = real_out.reshape(count, length) * factor
    return real_out[:, None, :]


def general_shards(tokens, proj_in, proj_out):
    seq_rows = tokens[0]
    local_len = seq_rows.shape[0]
    features = proj_in.shape[1]
    groups = features // GRP
    mapped = jnp.dot(
        seq_rows,
        lax.all_gather(proj_in, "col", axis=0, tiled=True),
        preferred_element_type=jnp.float32,
    ).astype(jnp.bfloat16)
    values = mapped.astype(jnp.float32).reshape(local_len, groups, GRP)
    cos_c, sin_c = circle(GRP, GRP, GRP)
    real_part = jnp.einsum("pgc,cs->gsp", values, cos_c, precision=highest)
    imag_part = jnp.einsum("pgc,cs->gsp", values, sin_c, precision=highest)
    ways = lax.axis_size("row")
    slots = groups * cos_c.shape[1]
    per_dev = slots // ways
    stacked = jnp.stack(
        [real_part.reshape(ways, per_dev, local_len), imag_part.reshape(ways, per_dev, local_len)],
        0,
    )
    spectra = positions(lax.all_to_all(stacked, "row", split_axis=1, concat_axis=3, tiled=True))
    outgoing = spectra.astype(jnp.bfloat16)
    back = lax.all_to_all(outgoing, "row", split_axis=2, concat_axis=0, tiled=True)
    mixed = back.reshape(features, local_len)
    result = lax.dot_general(
        mixed,
        lax.all_gather(proj_out, "row", axis=1, tiled=True),
        (((0,), (0,)), ((), ())),
        preferred_element_type=jnp.float32,
    )
    return result.astype(jnp.bfloat16)[None]


def channel_table(quarters, pairs):
    c = np.arange(GRP)
    rows = []
    for t in range(quarters):
        j = pairs * t + np.arange(pairs)
        angle = 2 * np.pi * (j[:, None] * c % GRP) / GRP
        sine = np.sin(angle)
        if t == 0:
            sine[0] = np.cos(np.pi * c)
        rows += [np.cos(angle), sine]
    return np.concatenate(rows, 0)


def channel_order(groups, quarters, pairs):
    order = []
    for g in range(groups):
        for t in range(quarters):
            j = pairs * t + np.arange(pairs)
            mirror = (GRP - j) % GRP
            if t == 0:
                mirror[0] = GRP // 2
            order += list(g * GRP + j) + list(g * GRP + mirror)
    return np.array(order)


def position_tables(ways, span):
    per = span // ways
    q = np.arange(span)
    low = min(LANES, span)
    even = np.zeros((ways, 16, 4 * LANES))
    odd = np.zeros((ways, 16, 4 * LANES))
    for owner in range(ways):
        for m in range(per):
            angle = 2 * np.pi * (q * (per * owner + m) % span) / span
            row = np.zeros(4 * LANES)
            row[:low] = np.cos(angle[:low])
            row[LANES : LANES + low] = np.sin(angle[:low])
            row[2 * LANES : 2 * LANES + span - low] = np.cos(angle[low:])
            row[3 * LANES : 3 * LANES + span - low] = np.sin(angle[low:])
            even[owner, m] = row
            odd[owner, m if m < 8 else m + 4] = row
    return even.reshape(-1, 4 * LANES), odd.reshape(-1, 4 * LANES)


def twiddle_table(ways, span):
    length = ways * span
    factor = 1.0 / math.sqrt(GRP * length)
    q = np.arange(2 * LANES)
    angle = 2 * np.pi * (np.arange(ways)[:, None] * q % length) / length
    cos, sin = np.cos(angle) * factor, np.sin(angle) * factor
    return np.stack([cos[:, :LANES], sin[:, :LANES], cos[:, LANES:], sin[:, LANES:]], 1)


def row_order(span):
    chunk = []
    chunk += [(0, m) for m in range(8)] + [(2, m) for m in range(8)]
    for a in range(4):
        chunk += [((0, 2, 1, 3)[a], 8 + m) for m in range(4)]
    chunk += [(1, m) for m in range(8)] + [(3, m) for m in range(8)]
    rows = len(chunk)
    hot = np.zeros((span, span))
    for b in range(4):
        for i, (a, m) in enumerate(chunk):
            hot[16 * m + 4 * a + b, b * rows + i] = 1
    return hot


def fetch_kernel(core, w_out, tok, w, table, mine, tok_copy, w_copy, table_copy, sems):
    half = mine.shape[0]
    rows = pl.ds(pl.multiple_of(core[0] * half, half), half)
    copies = [
        pltpu.make_async_copy(w_out.at[rows, :], mine, sems.at[0]),
        pltpu.make_async_copy(tok, tok_copy, sems.at[1]),
        pltpu.make_async_copy(w, w_copy, sems.at[2]),
        pltpu.make_async_copy(table, table_copy, sems.at[3]),
    ]
    for copy in copies:
        copy.start()
    for copy in copies:
        copy.wait()


def send_kernel(core, tok, w_own, w_other, table, out, padded):
    span, features = tok.shape[0], w_own.shape[1]
    depth = w_own.shape[0]
    columns = lambda which: pl.ds(pl.multiple_of(which * depth, depth), depth)
    mapped = jnp.dot(tok[:, columns(core[0])], w_own[...], preferred_element_type=jnp.float32) + jnp.dot(
        tok[:, columns(1 - core[0])], w_other[...], preferred_element_type=jnp.float32
    )
    padded[pl.ds(0, span), :] = mapped.astype(jnp.bfloat16)
    padded[pl.ds(span, 2 * LANES - span), :] = jnp.zeros((2 * LANES - span, features), jnp.bfloat16)
    groups = features // GRP
    quarters = out.shape[0] // groups
    for g in range(groups):
        turned = lax.dot_general(
            table[...],
            padded[:, g * GRP : (g + 1) * GRP],
            (((1,), (1,)), ((), ())),
            preferred_element_type=jnp.float32,
        )
        for t in range(quarters):
            cos = turned[32 * t : 32 * t + 16]
            sin = turned[32 * t + 16 : 32 * t + 32]
            high = cos[:, LANES:] + pltpu.roll(sin[:, LANES:], LANES // 2, 1)
            d = g * quarters + t
            out[d, 0:16, :] = cos[:, :LANES].astype(jnp.bfloat16)
            out[d, 16:32, :] = sin[:, :LANES].astype(jnp.bfloat16)
            out[d, 32:48, :] = high.astype(jnp.bfloat16)


def fft4(a, b, c, d):
    (ar, ai), (br, bi), (cr, ci), (dr, di) = a, b, c, d
    sr, si, tr, ti = ar + cr, ai + ci, ar - cr, ai - ci
    ur, ui, vr, vi = br + dr, bi + di, br - dr, bi - di
    return [(sr + ur, si + ui), (tr + vi, ti - vr), (sr - ur, si - ui), (tr - vi, ti + vr)]


def turn(v, n):
    re, im = v
    n %= 16
    if n == 0:
        return v
    if n == 4:
        return (im, -re)
    if n == 2:
        h = math.sqrt(0.5)
        return ((re + im) * h, (im - re) * h)
    if n == 6:
        h = math.sqrt(0.5)
        return ((im - re) * h, -(re + im) * h)
    c, s = math.cos(2 * math.pi * n / 16), math.sin(2 * math.pi * n / 16)
    return (re * c + im * s, im * c - re * s)


def fft16(v):
    inner = [fft4(v[a], v[a + 4], v[a + 8], v[a + 12]) for a in range(4)]
    out = [None] * 16
    for f in range(4):
        col = fft4(*[turn(inner[a][f], a * f) for a in range(4)])
        for e in range(4):
            out[f + 4 * e] = col[e]
    return out


def mix_kernel(special, x, even, odd, twist, out, turned):
    ways = x.shape[0]
    first = (lax.broadcasted_iota(jnp.int32, (16, LANES), 0) == 0) & (special[0] == 0)
    for part in range(2):
        v = []
        for r in range(ways):
            if part == 0:
                re = x[r, 0:16, :].astype(jnp.float32)
                im = -x[r, 16:32, :].astype(jnp.float32)
            else:
                re = x[r, 32:48, :].astype(jnp.float32)
                im = -pltpu.roll(re, LANES // 2, 1)
            v.append((re, im))
        spec = fft16(v)
        for k in range(ways):
            pr, pi = spec[k]
            qr, qi = spec[-k % ways]
            qi = -qi
            ur = jnp.where(first, (pr + qr) * 0.5, pr)
            ui = jnp.where(first, (pi + qi) * 0.5, pi)
            wr = jnp.where(first, (qi - pi) * 0.5, qr)
            wi = jnp.where(first, (pr - qr) * 0.5, qi)
            c = twist[k, 2 * part : 2 * part + 1, :]
            s = twist[k, 2 * part + 1 : 2 * part + 2, :]
            lo = slice(2 * part * LANES, (2 * part + 1) * LANES)
            hi = slice((2 * part + 1) * LANES, (2 * part + 2) * LANES)
            turned[32 * k : 32 * k + 16, lo] = (ur * c + ui * s).astype(jnp.bfloat16)
            turned[32 * k : 32 * k + 16, hi] = (ui * c - ur * s).astype(jnp.bfloat16)
            turned[32 * k + 16 : 32 * k + 32, lo] = (wr * c + wi * s).astype(jnp.bfloat16)
            turned[32 * k + 16 : 32 * k + 32, hi] = (wi * c - wr * s).astype(jnp.bfloat16)
    half = turned.shape[0] // 2
    nt = (((1,), (1,)), ((), ()))
    one = lax.dot_general(even[...], turned[:half, :], nt, preferred_element_type=jnp.float32)
    two = lax.dot_general(odd[...], turned[half:, :], nt, preferred_element_type=jnp.float32)
    for r in range(ways):
        e, o = one[16 * r : 16 * r + 16], two[16 * r : 16 * r + 16]
        tail = e[8:] + o[8:]
        left, right = slice(0, LANES), slice(LANES, 2 * LANES)
        out[r, 0:16, :] = jnp.concatenate([e[:8, left], o[:8, left]], 0).astype(jnp.bfloat16)
        out[r, 16:32, :] = jnp.concatenate([tail[:, left], tail[:, right]], 0).astype(jnp.bfloat16)
        out[r, 32:48, :] = jnp.concatenate([e[:8, right], o[:8, right]], 0).astype(jnp.bfloat16)


def gather_blocks(y, groups, stage):
    quarters = y.shape[0] // groups
    rows = y.shape[1]
    lane = lax.broadcasted_iota(jnp.int32, (rows, LANES), 1) // 32
    odd, high = lane % 2 == 1, lane >= 2
    for g in range(groups):
        v = [y[g * quarters + t].astype(jnp.float32) for t in range(quarters)]
        w = [None] * 4
        for t in (0, 2):
            w[t] = jnp.where(odd, pltpu.roll(v[t + 1], 32, 1), v[t])
            w[t + 1] = jnp.where(odd, v[t + 1], pltpu.roll(v[t], LANES - 32, 1))
        u = [None] * 4
        for b in (0, 1):
            u[b] = jnp.where(high, pltpu.roll(w[b + 2], 64, 1), w[b])
            u[b + 2] = jnp.where(high, w[b + 2], pltpu.roll(w[b], 64, 1))
        for b in range(4):
            stage[b * rows : (b + 1) * rows, g * GRP : (g + 1) * GRP] = u[b].astype(jnp.bfloat16)


def out_kernel(place, y, hot, swap, near, other, out, stage, mixed, held, sems):
    row, core = place[0], place[1]
    features = stage.shape[1]
    groups = features // GRP
    half = features // 2
    gather_blocks(y, groups, stage)
    rows = jnp.dot(hot[...], stage[...], preferred_element_type=jnp.float32).astype(jnp.bfloat16)
    for g in range(groups):
        part = slice(g * GRP, (g + 1) * GRP)
        mixed[:, part] = jnp.dot(rows[:, part], swap[...], preferred_element_type=jnp.float32).astype(jnp.bfloat16)
    left = mixed[:, pl.ds(pl.multiple_of(core * half, half), half)]
    right = mixed[:, pl.ds(pl.multiple_of((1 - core) * half, half), half)]
    ways = near.shape[0]
    copies = []
    for i in range(0, ways, 2):
        both = jnp.dot(
            left, jnp.concatenate([near[i], near[i + 1]], 1), preferred_element_type=jnp.float32
        ) + jnp.dot(right, jnp.concatenate([other[i], other[i + 1]], 1), preferred_element_type=jnp.float32)
        for n in range(2):
            plane, dz = (i + n) // (ways // 4), (i + n) % (ways // 4)
            owner = lax.bitwise_xor(lax.rem(row + 4 * dz, ways), plane)
            columns = pl.ds(pl.multiple_of(owner * LANES, LANES), LANES)
            held[:, columns] = both[:, n * LANES : (n + 1) * LANES].astype(jnp.bfloat16)
            copies.append(pltpu.make_async_copy(held.at[:, columns], out.at[:, columns], sems.at[i + n]))
            copies[-1].start()
    for copy in copies:
        copy.wait()


def vmem(count):
    return [pl.BlockSpec(memory_space=pltpu.VMEM)] * count


def shards(tokens, proj_in, proj_out):
    return fast_shards(tokens, proj_in, proj_out)


def fast_shards(tokens, proj_in, proj_out):
    seq_rows = tokens[0]
    span, _ = seq_rows.shape
    depth, features = proj_in.shape
    ways = lax.axis_size("row")
    groups = features // GRP
    quarters = ways // groups
    pairs = GRP // 2 // quarters
    bf16, f32 = jnp.bfloat16, jnp.float32
    room = pltpu.CompilerParams(vmem_limit_bytes=16 << 20)

    me = lax.axis_index("col")
    half = features // 2
    swap_cores = lambda v: lax.ppermute(v, "col", [(0, 1), (1, 0)])
    along = lambda v, to: lax.ppermute(v, ("row", "col"), [(2 * r + c, 2 * to(r, c) + c) for r in range(ways) for c in (0, 1)])
    other_w = swap_cores(proj_in)
    table = jnp.asarray(channel_table(quarters, pairs), bf16)
    hbm = pl.BlockSpec(memory_space=pltpu.MemorySpace.HBM)
    smem = pl.BlockSpec(memory_space=pltpu.SMEM)
    mine, tok, w_own, table = pl.pallas_call(
        fetch_kernel,
        in_specs=[smem] + [hbm] * 4,
        out_specs=vmem(4),
        out_shape=[
            jax.ShapeDtypeStruct((half, LANES), bf16),
            jax.ShapeDtypeStruct(seq_rows.shape, bf16),
            jax.ShapeDtypeStruct(proj_in.shape, bf16),
            jax.ShapeDtypeStruct(table.shape, bf16),
        ],
        scratch_shapes=[pltpu.SemaphoreType.DMA((4,))],
        compiler_params=room,
        name="fetch",
    )(me[None], *[pltpu.with_memory_space_constraint(v, pltpu.MemorySpace.HBM) for v in (proj_out, seq_rows, proj_in, table)])
    ring = [mine]
    for dz in range(1, ways // 4):
        ring.append(along(mine, lambda r, c: (r - 4 * dz) % ways))
    sent = pl.pallas_call(
        send_kernel,
        in_specs=[smem] + vmem(4),
        out_specs=vmem(1)[0],
        out_shape=jax.ShapeDtypeStruct((ways, 48, LANES), bf16),
        scratch_shapes=[pltpu.VMEM((2 * LANES, features), bf16)],
        cost_estimate=pl.CostEstimate(flops=2 * span * depth * features, bytes_accessed=2 << 20, transcendentals=0),
        compiler_params=room,
        name="send",
    )(me[None], tok, w_own, other_w, table)
    *ring, _ = lax.optimization_barrier((*ring, sent))
    ring = jnp.stack(ring, 0)
    planes = [along(ring, lambda r, c: r ^ flip) for flip in (1, 2, 3)]
    held = lax.all_to_all(sent, "row", 0, 0, tiled=True)

    even, odd = position_tables(ways, span)
    even, odd = jnp.asarray(even, bf16), jnp.asarray(odd, bf16)
    twist = jnp.asarray(twiddle_table(ways, span), f32)
    special = lax.rem(lax.axis_index("row"), quarters)[None]
    spectra = pl.pallas_call(
        mix_kernel,
        in_specs=[pl.BlockSpec(memory_space=pltpu.SMEM)] + vmem(4),
        out_specs=vmem(1)[0],
        out_shape=jax.ShapeDtypeStruct((ways, 48, LANES), bf16),
        scratch_shapes=[pltpu.VMEM((ways * 32, 4 * LANES), bf16)],
        compiler_params=room,
        name="mix",
    )(special, held, even, odd, twist)

    back = lax.all_to_all(spectra, "row", 0, 0, tiled=True)
    *planes, _ = lax.optimization_barrier((*planes, spectra))
    near = jnp.concatenate([ring] + planes, 0)
    other = swap_cores(near)
    hot = jnp.asarray(row_order(span), bf16)
    swap = np.zeros((GRP, GRP))
    swap[np.arange(GRP), channel_order(1, quarters, pairs)] = 1
    place = jnp.stack([lax.axis_index("row"), me])
    wide = ways * LANES
    result = pl.pallas_call(
        out_kernel,
        in_specs=[smem] + vmem(5),
        out_specs=hbm,
        out_shape=jax.ShapeDtypeStruct((span, wide), bf16),
        scratch_shapes=[
            pltpu.VMEM((span, features), bf16),
            pltpu.VMEM((span, features), bf16),
            pltpu.VMEM((span, wide), bf16),
            pltpu.SemaphoreType.DMA((ways,)),
        ],
        cost_estimate=pl.CostEstimate(flops=2 * span * wide * features, bytes_accessed=4 << 20, transcendentals=0),
        compiler_params=room,
        name="out",
    )(place, back, hot, jnp.asarray(swap, bf16), near, other)
    return result[None]


def fits(mesh, tokens, proj_in, proj_out):
    ways, cols = mesh.shape["row"], mesh.shape["col"]
    features = proj_in.shape[1]
    span = tokens.shape[1] // ways
    return (
        features % GRP == 0
        and ways == 4 * (features // GRP) == 16
        and span == 12 * ways
        and cols == 2
        and tokens.shape[0] == cols
        and proj_out.shape[1] == ways * LANES
    )


def solution(mesh):
    in_specs = (P("col", "row", None), P("col", None), P(None, "row"))
    out_specs = P("col", "row", None)

    def run(tokens, proj_in, proj_out):
        fast = fits(mesh, tokens, proj_in, proj_out)
        body = shards if fast else general_shards
        step = jax.shard_map(body, mesh=mesh, in_specs=in_specs, out_specs=out_specs, check_vma=False)
        return step(tokens, proj_in, proj_out)

    return run
```

```python
import math

import jax
import jax.numpy as jnp
import numpy as np
from jax import lax
from jax.experimental import pallas as pl
from jax.experimental.pallas import tpu as pltpu
from jax.sharding import PartitionSpec as P


GRP = 128
LANES = 128
highest = lax.Precision.HIGHEST
span_inner = 128


def circle(height, breadth, period):
    product = lax.iota(jnp.int32, height)[:, None] * lax.iota(jnp.int32, breadth)[None, :] % period
    angle = product.astype(jnp.float32) * (2.0 * math.pi / period)
    return (jnp.cos(angle), jnp.sin(angle))


def positions(piece):
    real_in = piece[0, 0]
    imag_in = piece[1, 0]
    count, length = real_in.shape
    outer = length // span_inner
    real_in = real_in.reshape(count, outer, span_inner)
    imag_in = imag_in.reshape(count, outer, span_inner)
    cos_one, sin_one = circle(outer, outer, outer)
    first_re = jnp.einsum("ab,kbq->kaq", cos_one, real_in, precision=highest) - jnp.einsum(
        "ab,kbq->kaq", sin_one, imag_in, precision=highest
    )
    first_im = jnp.einsum("ab,kbq->kaq", sin_one, real_in, precision=highest) + jnp.einsum(
        "ab,kbq->kaq", cos_one, imag_in, precision=highest
    )
    twist_c, twist_s = circle(outer, span_inner, length)
    turned_re = first_re * twist_c - first_im * twist_s
    turned_im = first_re * twist_s + first_im * twist_c
    cos_two, sin_two = circle(span_inner, span_inner, span_inner)
    factor = 1.0 / math.sqrt(GRP * length)
    real_out = jnp.einsum("kaq,qb->kba", turned_re, cos_two, precision=highest) - jnp.einsum(
        "kaq,qb->kba", turned_im, sin_two, precision=highest
    )
    real_out = real_out.reshape(count, length) * factor
    return real_out[:, None, :]


def general_shards(tokens, proj_in, proj_out):
    seq_rows = tokens[0]
    local_len = seq_rows.shape[0]
    features = proj_in.shape[1]
    groups = features // GRP
    mapped = jnp.dot(
        seq_rows,
        lax.all_gather(proj_in, "col", axis=0, tiled=True),
        preferred_element_type=jnp.float32,
    ).astype(jnp.bfloat16)
    values = mapped.astype(jnp.float32).reshape(local_len, groups, GRP)
    cos_c, sin_c = circle(GRP, GRP, GRP)
    real_part = jnp.einsum("pgc,cs->gsp", values, cos_c, precision=highest)
    imag_part = jnp.einsum("pgc,cs->gsp", values, sin_c, precision=highest)
    ways = lax.axis_size("row")
    slots = groups * cos_c.shape[1]
    per_dev = slots // ways
    stacked = jnp.stack(
        [real_part.reshape(ways, per_dev, local_len), imag_part.reshape(ways, per_dev, local_len)],
        0,
    )
    spectra = positions(lax.all_to_all(stacked, "row", split_axis=1, concat_axis=3, tiled=True))
    outgoing = spectra.astype(jnp.bfloat16)
    back = lax.all_to_all(outgoing, "row", split_axis=2, concat_axis=0, tiled=True)
    mixed = back.reshape(features, local_len)
    result = lax.dot_general(
        mixed,
        lax.all_gather(proj_out, "row", axis=1, tiled=True),
        (((0,), (0,)), ((), ())),
        preferred_element_type=jnp.float32,
    )
    return result.astype(jnp.bfloat16)[None]


def channel_table(quarters, pairs):
    c = np.arange(GRP)
    rows = []
    for t in range(quarters):
        j = pairs * t + np.arange(pairs)
        angle = 2 * np.pi * (j[:, None] * c % GRP) / GRP
        sine = np.sin(angle)
        if t == 0:
            sine[0] = np.cos(np.pi * c)
        rows += [np.cos(angle), sine]
    return np.concatenate(rows, 0)


def channel_order(groups, quarters, pairs):
    order = []
    for g in range(groups):
        for t in range(quarters):
            j = pairs * t + np.arange(pairs)
            mirror = (GRP - j) % GRP
            if t == 0:
                mirror[0] = GRP // 2
            order += list(g * GRP + j) + list(g * GRP + mirror)
    return np.array(order)


def position_tables(ways, span):
    per = span // ways
    q = np.arange(span)
    low = min(LANES, span)
    even = np.zeros((ways, 16, 4 * LANES))
    odd = np.zeros((ways, 16, 4 * LANES))
    for owner in range(ways):
        for m in range(per):
            angle = 2 * np.pi * (q * (per * owner + m) % span) / span
            row = np.zeros(4 * LANES)
            row[:low] = np.cos(angle[:low])
            row[LANES : LANES + low] = np.sin(angle[:low])
            row[2 * LANES : 2 * LANES + span - low] = np.cos(angle[low:])
            row[3 * LANES : 3 * LANES + span - low] = np.sin(angle[low:])
            even[owner, m] = row
            odd[owner, m if m < 8 else m + 4] = row
    return even.reshape(-1, 4 * LANES), odd.reshape(-1, 4 * LANES)


def twiddle_table(ways, span):
    length = ways * span
    factor = 1.0 / math.sqrt(GRP * length)
    q = np.arange(2 * LANES)
    angle = 2 * np.pi * (np.arange(ways)[:, None] * q % length) / length
    cos, sin = np.cos(angle) * factor, np.sin(angle) * factor
    return np.stack([cos[:, :LANES], sin[:, :LANES], cos[:, LANES:], sin[:, LANES:]], 1)


def row_order(span):
    chunk = []
    chunk += [(0, m) for m in range(8)] + [(2, m) for m in range(8)]
    for a in range(4):
        chunk += [((0, 2, 1, 3)[a], 8 + m) for m in range(4)]
    chunk += [(1, m) for m in range(8)] + [(3, m) for m in range(8)]
    rows = len(chunk)
    hot = np.zeros((span, span))
    for b in range(4):
        for i, (a, m) in enumerate(chunk):
            hot[16 * m + 4 * a + b, b * rows + i] = 1
    return hot


def fetch_kernel(core, w_out, swap, w, table, mine, w_copy, table_copy, raw, hot, sems):
    half = mine.shape[0]
    rows = pl.ds(pl.multiple_of(core[0] * half, half), half)
    copies = [
        pltpu.make_async_copy(w_out.at[rows, :], raw, sems.at[0]),
        pltpu.make_async_copy(swap, hot, sems.at[1]),
        pltpu.make_async_copy(w, w_copy, sems.at[2]),
        pltpu.make_async_copy(table, table_copy, sems.at[3]),
    ]
    for copy in copies:
        copy.start()
    copies[0].wait()
    copies[1].wait()
    for g in range(half // GRP):
        part = slice(g * GRP, (g + 1) * GRP)
        mine[part, :] = jnp.dot(hot[...], raw[part, :], preferred_element_type=jnp.float32).astype(jnp.bfloat16)
    for copy in copies[2:]:
        copy.wait()


def send_kernel(core, tok, w_own, w_other, table, out, padded):
    span, features = tok.shape[0], w_own.shape[1]
    depth = w_own.shape[0]
    columns = lambda which: pl.ds(pl.multiple_of(which * depth, depth), depth)
    mapped = jnp.dot(tok[:, columns(core[0])], w_own[...], preferred_element_type=jnp.float32) + jnp.dot(
        tok[:, columns(1 - core[0])], w_other[...], preferred_element_type=jnp.float32
    )
    padded[pl.ds(0, span), :] = mapped.astype(jnp.bfloat16)
    padded[pl.ds(span, 2 * LANES - span), :] = jnp.zeros((2 * LANES - span, features), jnp.bfloat16)
    groups = features // GRP
    quarters = out.shape[0] // groups
    for g in range(groups):
        turned = lax.dot_general(
            table[...],
            padded[:, g * GRP : (g + 1) * GRP],
            (((1,), (1,)), ((), ())),
            preferred_element_type=jnp.float32,
        )
        for t in range(quarters):
            cos = turned[32 * t : 32 * t + 16]
            sin = turned[32 * t + 16 : 32 * t + 32]
            high = cos[:, LANES:] + pltpu.roll(sin[:, LANES:], LANES // 2, 1)
            d = g * quarters + t
            out[d, 0:16, :] = cos[:, :LANES].astype(jnp.bfloat16)
            out[d, 16:32, :] = sin[:, :LANES].astype(jnp.bfloat16)
            out[d, 32:48, :] = high.astype(jnp.bfloat16)


def fft4(a, b, c, d):
    (ar, ai), (br, bi), (cr, ci), (dr, di) = a, b, c, d
    sr, si, tr, ti = ar + cr, ai + ci, ar - cr, ai - ci
    ur, ui, vr, vi = br + dr, bi + di, br - dr, bi - di
    return [(sr + ur, si + ui), (tr + vi, ti - vr), (sr - ur, si - ui), (tr - vi, ti + vr)]


def turn(v, n):
    re, im = v
    n %= 16
    if n == 0:
        return v
    if n == 4:
        return (im, -re)
    if n == 2:
        h = math.sqrt(0.5)
        return ((re + im) * h, (im - re) * h)
    if n == 6:
        h = math.sqrt(0.5)
        return ((im - re) * h, -(re + im) * h)
    c, s = math.cos(2 * math.pi * n / 16), math.sin(2 * math.pi * n / 16)
    return (re * c + im * s, im * c - re * s)


def fft16(v):
    inner = [fft4(v[a], v[a + 4], v[a + 8], v[a + 12]) for a in range(4)]
    out = [None] * 16
    for f in range(4):
        col = fft4(*[turn(inner[a][f], a * f) for a in range(4)])
        for e in range(4):
            out[f + 4 * e] = col[e]
    return out


def mix_kernel(special, x, even, odd, twist, out, turned):
    ways = x.shape[0]
    first = (lax.broadcasted_iota(jnp.int32, (16, LANES), 0) == 0) & (special[0] == 0)
    for part in range(2):
        v = []
        for r in range(ways):
            if part == 0:
                re = x[r, 0:16, :].astype(jnp.float32)
                im = -x[r, 16:32, :].astype(jnp.float32)
            else:
                re = x[r, 32:48, :].astype(jnp.float32)
                im = -pltpu.roll(re, LANES // 2, 1)
            v.append((re, im))
        spec = fft16(v)
        for k in range(ways):
            pr, pi = spec[k]
            qr, qi = spec[-k % ways]
            qi = -qi
            ur = jnp.where(first, (pr + qr) * 0.5, pr)
            ui = jnp.where(first, (pi + qi) * 0.5, pi)
            wr = jnp.where(first, (qi - pi) * 0.5, qr)
            wi = jnp.where(first, (pr - qr) * 0.5, qi)
            c = twist[k, 2 * part : 2 * part + 1, :]
            s = twist[k, 2 * part + 1 : 2 * part + 2, :]
            lo = slice(2 * part * LANES, (2 * part + 1) * LANES)
            hi = slice((2 * part + 1) * LANES, (2 * part + 2) * LANES)
            turned[32 * k : 32 * k + 16, lo] = (ur * c + ui * s).astype(jnp.bfloat16)
            turned[32 * k : 32 * k + 16, hi] = (ui * c - ur * s).astype(jnp.bfloat16)
            turned[32 * k + 16 : 32 * k + 32, lo] = (wr * c + wi * s).astype(jnp.bfloat16)
            turned[32 * k + 16 : 32 * k + 32, hi] = (wi * c - wr * s).astype(jnp.bfloat16)
    half = turned.shape[0] // 2
    nt = (((1,), (1,)), ((), ()))
    one = lax.dot_general(even[...], turned[:half, :], nt, preferred_element_type=jnp.float32)
    two = lax.dot_general(odd[...], turned[half:, :], nt, preferred_element_type=jnp.float32)
    for r in range(ways):
        e, o = one[16 * r : 16 * r + 16], two[16 * r : 16 * r + 16]
        tail = e[8:] + o[8:]
        left, right = slice(0, LANES), slice(LANES, 2 * LANES)
        out[r, 0:16, :] = jnp.concatenate([e[:8, left], o[:8, left]], 0).astype(jnp.bfloat16)
        out[r, 16:32, :] = jnp.concatenate([tail[:, left], tail[:, right]], 0).astype(jnp.bfloat16)
        out[r, 32:48, :] = jnp.concatenate([e[:8, right], o[:8, right]], 0).astype(jnp.bfloat16)


def gather_blocks(y, groups, stage):
    quarters = y.shape[0] // groups
    rows = y.shape[1]
    lane = lax.broadcasted_iota(jnp.int32, (rows, LANES), 1) // 32
    odd, high = lane % 2 == 1, lane >= 2
    for g in range(groups):
        v = [y[g * quarters + t].astype(jnp.float32) for t in range(quarters)]
        w = [None] * 4
        for t in (0, 2):
            w[t] = jnp.where(odd, pltpu.roll(v[t + 1], 32, 1), v[t])
            w[t + 1] = jnp.where(odd, v[t + 1], pltpu.roll(v[t], LANES - 32, 1))
        u = [None] * 4
        for b in (0, 1):
            u[b] = jnp.where(high, pltpu.roll(w[b + 2], 64, 1), w[b])
            u[b + 2] = jnp.where(high, w[b + 2], pltpu.roll(w[b], 64, 1))
        for b in range(4):
            stage[b * rows : (b + 1) * rows, g * GRP : (g + 1) * GRP] = u[b].astype(jnp.bfloat16)


def out_kernel(place, y, hot, near, other, far, far_other, out, stage, mixed, held, sems):
    row, core = place[0], place[1]
    features = stage.shape[1]
    groups = features // GRP
    half = features // 2
    gather_blocks(y, groups, stage)
    mixed[...] = jnp.dot(hot[...], stage[...], preferred_element_type=jnp.float32).astype(jnp.bfloat16)
    left = mixed[:, pl.ds(pl.multiple_of(core * half, half), half)]
    right = mixed[:, pl.ds(pl.multiple_of((1 - core) * half, half), half)]
    count = near.shape[0]
    ways = count + far.shape[0]
    copies = []
    for i in range(0, ways, 2):
        ours, theirs, at = (near, other, i) if i < count else (far, far_other, i - count)
        both = jnp.dot(
            left, jnp.concatenate([ours[at], ours[at + 1]], 1), preferred_element_type=jnp.float32
        ) + jnp.dot(right, jnp.concatenate([theirs[at], theirs[at + 1]], 1), preferred_element_type=jnp.float32)
        for n in range(2):
            plane, dz = (1, 2, 0, 3)[(i + n) // (ways // 4)], (i + n) % (ways // 4)
            owner = lax.bitwise_xor(lax.rem(row + 4 * dz, ways), plane)
            columns = pl.ds(pl.multiple_of(owner * LANES, LANES), LANES)
            held[:, columns] = both[:, n * LANES : (n + 1) * LANES].astype(jnp.bfloat16)
            copies.append(pltpu.make_async_copy(held.at[:, columns], out.at[:, columns], sems.at[i + n]))
            copies[-1].start()
    for copy in copies:
        copy.wait()


def vmem(count):
    return [pl.BlockSpec(memory_space=pltpu.VMEM)] * count


def shards(tokens, proj_in, proj_out):
    return fast_shards(tokens, proj_in, proj_out)


def fast_shards(tokens, proj_in, proj_out):
    seq_rows = tokens[0]
    span, _ = seq_rows.shape
    depth, features = proj_in.shape
    ways = lax.axis_size("row")
    groups = features // GRP
    quarters = ways // groups
    pairs = GRP // 2 // quarters
    bf16, f32 = jnp.bfloat16, jnp.float32
    room = pltpu.CompilerParams(vmem_limit_bytes=16 << 20)

    me = lax.axis_index("col")
    half = features // 2
    swap_cores = lambda v: lax.ppermute(v, "col", [(0, 1), (1, 0)])
    along = lambda v, to: lax.ppermute(v, ("row", "col"), [(2 * r + c, 2 * to(r, c) + c) for r in range(ways) for c in (0, 1)])
    other_w = swap_cores(proj_in)
    table = jnp.asarray(channel_table(quarters, pairs), bf16)
    swap = np.zeros((GRP, GRP))
    swap[np.arange(GRP), channel_order(1, quarters, pairs)] = 1
    swap = jnp.asarray(swap, bf16)
    hbm = pl.BlockSpec(memory_space=pltpu.MemorySpace.HBM)
    smem = pl.BlockSpec(memory_space=pltpu.SMEM)
    mine, w_own, table = pl.pallas_call(
        fetch_kernel,
        in_specs=[smem] + [hbm] * 4,
        out_specs=vmem(3),
        out_shape=[
            jax.ShapeDtypeStruct((half, LANES), bf16),
            jax.ShapeDtypeStruct(proj_in.shape, bf16),
            jax.ShapeDtypeStruct(table.shape, bf16),
        ],
        scratch_shapes=[
            pltpu.VMEM((half, LANES), bf16),
            pltpu.VMEM((GRP, GRP), bf16),
            pltpu.SemaphoreType.DMA((4,)),
        ],
        compiler_params=room,
        name="fetch",
    )(me[None], *[pltpu.with_memory_space_constraint(v, pltpu.MemorySpace.HBM) for v in (proj_out, swap, proj_in, table)])
    ring = [mine]
    for dz in range(1, ways // 4):
        ring.append(along(mine, lambda r, c: (r - 4 * dz) % ways))
    sent = pl.pallas_call(
        send_kernel,
        in_specs=[smem] + vmem(4),
        out_specs=vmem(1)[0],
        out_shape=jax.ShapeDtypeStruct((ways, 48, LANES), bf16),
        scratch_shapes=[pltpu.VMEM((2 * LANES, features), bf16)],
        cost_estimate=pl.CostEstimate(flops=2 * span * depth * features, bytes_accessed=2 << 20, transcendentals=0),
        compiler_params=room,
        name="send",
    )(me[None], seq_rows, w_own, other_w, table)
    *ring, _ = lax.optimization_barrier((*ring, sent))
    ring = jnp.stack(ring, 0)
    planes = []
    for flip in (1, 2, 3):
        planes.append(along(ring, lambda r, c: r ^ flip))
    held = lax.all_to_all(sent, "row", 0, 0, tiled=True)

    even, odd = position_tables(ways, span)
    even, odd = jnp.asarray(even, bf16), jnp.asarray(odd, bf16)
    twist = jnp.asarray(twiddle_table(ways, span), f32)
    special = lax.rem(lax.axis_index("row"), quarters)[None]
    spectra = pl.pallas_call(
        mix_kernel,
        in_specs=[pl.BlockSpec(memory_space=pltpu.SMEM)] + vmem(4),
        out_specs=vmem(1)[0],
        out_shape=jax.ShapeDtypeStruct((ways, 48, LANES), bf16),
        scratch_shapes=[pltpu.VMEM((ways * 32, 4 * LANES), bf16)],
        compiler_params=room,
        name="mix",
    )(special, held, even, odd, twist)

    back = lax.all_to_all(spectra, "row", 0, 0, tiled=True)
    *planes, _ = lax.optimization_barrier((*planes, spectra))
    near = jnp.concatenate(planes[:2], 0)
    far = jnp.concatenate([ring, planes[2]], 0)
    other = swap_cores(near)
    far_other = swap_cores(far)
    hot = jnp.asarray(row_order(span), bf16)
    place = jnp.stack([lax.axis_index("row"), me])
    wide = ways * LANES
    result = pl.pallas_call(
        out_kernel,
        in_specs=[smem] + vmem(6),
        out_specs=hbm,
        out_shape=jax.ShapeDtypeStruct((span, wide), bf16),
        scratch_shapes=[
            pltpu.VMEM((span, features), bf16),
            pltpu.VMEM((span, features), bf16),
            pltpu.VMEM((span, wide), bf16),
            pltpu.SemaphoreType.DMA((ways,)),
        ],
        cost_estimate=pl.CostEstimate(flops=2 * span * wide * features, bytes_accessed=4 << 20, transcendentals=0),
        compiler_params=room,
        name="out",
    )(place, back, hot, near, other, far, far_other)
    return result[None]


def fits(mesh, tokens, proj_in, proj_out):
    ways, cols = mesh.shape["row"], mesh.shape["col"]
    features = proj_in.shape[1]
    span = tokens.shape[1] // ways
    return (
        features % GRP == 0
        and ways == 4 * (features // GRP) == 16
        and span == 12 * ways
        and cols == 2
        and tokens.shape[0] == cols
        and proj_out.shape[1] == ways * LANES
    )


def solution(mesh):
    in_specs = (P("col", "row", None), P("col", None), P(None, "row"))
    out_specs = P("col", "row", None)

    def run(tokens, proj_in, proj_out):
        fast = fits(mesh, tokens, proj_in, proj_out)
        body = shards if fast else general_shards
        step = jax.shard_map(body, mesh=mesh, in_specs=in_specs, out_specs=out_specs, check_vma=False)
        return step(tokens, proj_in, proj_out)

    return run
```

```python
import math

import jax
import jax.numpy as jnp
import numpy as np
from jax import lax
from jax.experimental import pallas as pl
from jax.experimental.pallas import tpu as pltpu
from jax.sharding import PartitionSpec as P


GRP = 128
LANES = 128
highest = lax.Precision.HIGHEST
span_inner = 128


def circle(height, breadth, period):
    product = lax.iota(jnp.int32, height)[:, None] * lax.iota(jnp.int32, breadth)[None, :] % period
    angle = product.astype(jnp.float32) * (2.0 * math.pi / period)
    return (jnp.cos(angle), jnp.sin(angle))


def positions(piece):
    real_in = piece[0, 0]
    imag_in = piece[1, 0]
    count, length = real_in.shape
    outer = length // span_inner
    real_in = real_in.reshape(count, outer, span_inner)
    imag_in = imag_in.reshape(count, outer, span_inner)
    cos_one, sin_one = circle(outer, outer, outer)
    first_re = jnp.einsum("ab,kbq->kaq", cos_one, real_in, precision=highest) - jnp.einsum(
        "ab,kbq->kaq", sin_one, imag_in, precision=highest
    )
    first_im = jnp.einsum("ab,kbq->kaq", sin_one, real_in, precision=highest) + jnp.einsum(
        "ab,kbq->kaq", cos_one, imag_in, precision=highest
    )
    twist_c, twist_s = circle(outer, span_inner, length)
    turned_re = first_re * twist_c - first_im * twist_s
    turned_im = first_re * twist_s + first_im * twist_c
    cos_two, sin_two = circle(span_inner, span_inner, span_inner)
    factor = 1.0 / math.sqrt(GRP * length)
    real_out = jnp.einsum("kaq,qb->kba", turned_re, cos_two, precision=highest) - jnp.einsum(
        "kaq,qb->kba", turned_im, sin_two, precision=highest
    )
    real_out = real_out.reshape(count, length) * factor
    return real_out[:, None, :]


def general_shards(tokens, proj_in, proj_out):
    seq_rows = tokens[0]
    local_len = seq_rows.shape[0]
    features = proj_in.shape[1]
    groups = features // GRP
    mapped = jnp.dot(
        seq_rows,
        lax.all_gather(proj_in, "col", axis=0, tiled=True),
        preferred_element_type=jnp.float32,
    ).astype(jnp.bfloat16)
    values = mapped.astype(jnp.float32).reshape(local_len, groups, GRP)
    cos_c, sin_c = circle(GRP, GRP, GRP)
    real_part = jnp.einsum("pgc,cs->gsp", values, cos_c, precision=highest)
    imag_part = jnp.einsum("pgc,cs->gsp", values, sin_c, precision=highest)
    ways = lax.axis_size("row")
    slots = groups * cos_c.shape[1]
    per_dev = slots // ways
    stacked = jnp.stack(
        [real_part.reshape(ways, per_dev, local_len), imag_part.reshape(ways, per_dev, local_len)],
        0,
    )
    spectra = positions(lax.all_to_all(stacked, "row", split_axis=1, concat_axis=3, tiled=True))
    outgoing = spectra.astype(jnp.bfloat16)
    back = lax.all_to_all(outgoing, "row", split_axis=2, concat_axis=0, tiled=True)
    mixed = back.reshape(features, local_len)
    result = lax.dot_general(
        mixed,
        lax.all_gather(proj_out, "row", axis=1, tiled=True),
        (((0,), (0,)), ((), ())),
        preferred_element_type=jnp.float32,
    )
    return result.astype(jnp.bfloat16)[None]


def channel_table(quarters, pairs):
    c = np.arange(GRP)
    rows = []
    for t in range(quarters):
        j = pairs * t + np.arange(pairs)
        angle = 2 * np.pi * (j[:, None] * c % GRP) / GRP
        sine = np.sin(angle)
        if t == 0:
            sine[0] = np.cos(np.pi * c)
        rows += [np.cos(angle), sine]
    return np.concatenate(rows, 0)


def channel_order(groups, quarters, pairs):
    order = []
    for g in range(groups):
        for t in range(quarters):
            j = pairs * t + np.arange(pairs)
            mirror = (GRP - j) % GRP
            if t == 0:
                mirror[0] = GRP // 2
            order += list(g * GRP + j) + list(g * GRP + mirror)
    return np.array(order)


def position_tables(ways, span):
    per = span // ways
    q = np.arange(span)
    low = min(LANES, span)
    even = np.zeros((ways, 16, 4 * LANES))
    odd = np.zeros((ways, 16, 4 * LANES))
    for owner in range(ways):
        for m in range(per):
            angle = 2 * np.pi * (q * (per * owner + m) % span) / span
            row = np.zeros(4 * LANES)
            row[:low] = np.cos(angle[:low])
            row[LANES : LANES + low] = np.sin(angle[:low])
            row[2 * LANES : 2 * LANES + span - low] = np.cos(angle[low:])
            row[3 * LANES : 3 * LANES + span - low] = np.sin(angle[low:])
            even[owner, m] = row
            odd[owner, m if m < 8 else m + 4] = row
    return even.reshape(-1, 4 * LANES), odd.reshape(-1, 4 * LANES)


def twiddle_table(ways, span):
    length = ways * span
    factor = 1.0 / math.sqrt(GRP * length)
    q = np.arange(2 * LANES)
    angle = 2 * np.pi * (np.arange(ways)[:, None] * q % length) / length
    cos, sin = np.cos(angle) * factor, np.sin(angle) * factor
    return np.stack([cos[:, :LANES], sin[:, :LANES], cos[:, LANES:], sin[:, LANES:]], 1)


def row_order(span):
    chunk = []
    chunk += [(0, m) for m in range(8)] + [(2, m) for m in range(8)]
    for a in range(4):
        chunk += [((0, 2, 1, 3)[a], 8 + m) for m in range(4)]
    chunk += [(1, m) for m in range(8)] + [(3, m) for m in range(8)]
    rows = len(chunk)
    hot = np.zeros((span, span))
    for b in range(4):
        for i, (a, m) in enumerate(chunk):
            hot[16 * m + 4 * a + b, b * rows + i] = 1
    return hot


def fetch_kernel(core, w_out, swap, mine, raw, hot, sems):
    half = mine.shape[0]
    rows = pl.ds(pl.multiple_of(core[0] * half, half), half)
    copies = [
        pltpu.make_async_copy(w_out.at[rows, :], raw, sems.at[0]),
        pltpu.make_async_copy(swap, hot, sems.at[1]),
    ]
    for copy in copies:
        copy.start()
    for copy in copies:
        copy.wait()
    for g in range(half // GRP):
        part = slice(g * GRP, (g + 1) * GRP)
        mine[part, :] = jnp.dot(hot[...], raw[part, :], preferred_element_type=jnp.float32).astype(jnp.bfloat16)


def send_kernel(core, tok, w_own, w_other, table, out, padded):
    span, features = tok.shape[0], w_own.shape[1]
    depth = w_own.shape[0]
    columns = lambda which: pl.ds(pl.multiple_of(which * depth, depth), depth)
    mapped = jnp.dot(tok[:, columns(core[0])], w_own[...], preferred_element_type=jnp.float32) + jnp.dot(
        tok[:, columns(1 - core[0])], w_other[...], preferred_element_type=jnp.float32
    )
    padded[pl.ds(0, span), :] = mapped.astype(jnp.bfloat16)
    padded[pl.ds(span, 2 * LANES - span), :] = jnp.zeros((2 * LANES - span, features), jnp.bfloat16)
    groups = features // GRP
    quarters = out.shape[0] // groups
    for g in range(groups):
        turned = lax.dot_general(
            table[...],
            padded[:, g * GRP : (g + 1) * GRP],
            (((1,), (1,)), ((), ())),
            preferred_element_type=jnp.float32,
        )
        for t in range(quarters):
            cos = turned[32 * t : 32 * t + 16]
            sin = turned[32 * t + 16 : 32 * t + 32]
            high = cos[:, LANES:] + pltpu.roll(sin[:, LANES:], LANES // 2, 1)
            d = g * quarters + t
            out[d, 0:16, :] = cos[:, :LANES].astype(jnp.bfloat16)
            out[d, 16:32, :] = sin[:, :LANES].astype(jnp.bfloat16)
            out[d, 32:48, :] = high.astype(jnp.bfloat16)


def fft4(a, b, c, d):
    (ar, ai), (br, bi), (cr, ci), (dr, di) = a, b, c, d
    sr, si, tr, ti = ar + cr, ai + ci, ar - cr, ai - ci
    ur, ui, vr, vi = br + dr, bi + di, br - dr, bi - di
    return [(sr + ur, si + ui), (tr + vi, ti - vr), (sr - ur, si - ui), (tr - vi, ti + vr)]


def turn(v, n):
    re, im = v
    n %= 16
    if n == 0:
        return v
    if n == 4:
        return (im, -re)
    if n == 2:
        h = math.sqrt(0.5)
        return ((re + im) * h, (im - re) * h)
    if n == 6:
        h = math.sqrt(0.5)
        return ((im - re) * h, -(re + im) * h)
    c, s = math.cos(2 * math.pi * n / 16), math.sin(2 * math.pi * n / 16)
    return (re * c + im * s, im * c - re * s)


def fft16(v):
    inner = [fft4(v[a], v[a + 4], v[a + 8], v[a + 12]) for a in range(4)]
    out = [None] * 16
    for f in range(4):
        col = fft4(*[turn(inner[a][f], a * f) for a in range(4)])
        for e in range(4):
            out[f + 4 * e] = col[e]
    return out


def mix_kernel(special, x, even, odd, twist, out, turned):
    ways = x.shape[0]
    first = (lax.broadcasted_iota(jnp.int32, (16, LANES), 0) == 0) & (special[0] == 0)
    for part in range(2):
        v = []
        for r in range(ways):
            if part == 0:
                re = x[r, 0:16, :].astype(jnp.float32)
                im = -x[r, 16:32, :].astype(jnp.float32)
            else:
                re = x[r, 32:48, :].astype(jnp.float32)
                im = -pltpu.roll(re, LANES // 2, 1)
            v.append((re, im))
        spec = fft16(v)
        for k in range(ways):
            pr, pi = spec[k]
            qr, qi = spec[-k % ways]
            qi = -qi
            ur = jnp.where(first, (pr + qr) * 0.5, pr)
            ui = jnp.where(first, (pi + qi) * 0.5, pi)
            wr = jnp.where(first, (qi - pi) * 0.5, qr)
            wi = jnp.where(first, (pr - qr) * 0.5, qi)
            c = twist[k, 2 * part : 2 * part + 1, :]
            s = twist[k, 2 * part + 1 : 2 * part + 2, :]
            lo = slice(2 * part * LANES, (2 * part + 1) * LANES)
            hi = slice((2 * part + 1) * LANES, (2 * part + 2) * LANES)
            turned[32 * k : 32 * k + 16, lo] = (ur * c + ui * s).astype(jnp.bfloat16)
            turned[32 * k : 32 * k + 16, hi] = (ui * c - ur * s).astype(jnp.bfloat16)
            turned[32 * k + 16 : 32 * k + 32, lo] = (wr * c + wi * s).astype(jnp.bfloat16)
            turned[32 * k + 16 : 32 * k + 32, hi] = (wi * c - wr * s).astype(jnp.bfloat16)
    half = turned.shape[0] // 2
    nt = (((1,), (1,)), ((), ()))
    one = lax.dot_general(even[...], turned[:half, :], nt, preferred_element_type=jnp.float32)
    two = lax.dot_general(odd[...], turned[half:, :], nt, preferred_element_type=jnp.float32)
    for r in range(ways):
        e, o = one[16 * r : 16 * r + 16], two[16 * r : 16 * r + 16]
        tail = e[8:] + o[8:]
        left, right = slice(0, LANES), slice(LANES, 2 * LANES)
        out[r, 0:16, :] = jnp.concatenate([e[:8, left], o[:8, left]], 0).astype(jnp.bfloat16)
        out[r, 16:32, :] = jnp.concatenate([tail[:, left], tail[:, right]], 0).astype(jnp.bfloat16)
        out[r, 32:48, :] = jnp.concatenate([e[:8, right], o[:8, right]], 0).astype(jnp.bfloat16)


def gather_blocks(y, groups, stage):
    quarters = y.shape[0] // groups
    rows = y.shape[1]
    lane = lax.broadcasted_iota(jnp.int32, (rows, LANES), 1) // 32
    odd, high = lane % 2 == 1, lane >= 2
    for g in range(groups):
        v = [y[g * quarters + t].astype(jnp.float32) for t in range(quarters)]
        w = [None] * 4
        for t in (0, 2):
            w[t] = jnp.where(odd, pltpu.roll(v[t + 1], 32, 1), v[t])
            w[t + 1] = jnp.where(odd, v[t + 1], pltpu.roll(v[t], LANES - 32, 1))
        u = [None] * 4
        for b in (0, 1):
            u[b] = jnp.where(high, pltpu.roll(w[b + 2], 64, 1), w[b])
            u[b + 2] = jnp.where(high, w[b + 2], pltpu.roll(w[b], 64, 1))
        for b in range(4):
            stage[b * rows : (b + 1) * rows, g * GRP : (g + 1) * GRP] = u[b].astype(jnp.bfloat16)


def out_kernel(place, y, hot, near, other, far, far_other, out, stage, mixed, held, sems):
    row, core = place[0], place[1]
    features = stage.shape[1]
    groups = features // GRP
    half = features // 2
    gather_blocks(y, groups, stage)
    mixed[...] = jnp.dot(hot[...], stage[...], preferred_element_type=jnp.float32).astype(jnp.bfloat16)
    left = mixed[:, pl.ds(pl.multiple_of(core * half, half), half)]
    right = mixed[:, pl.ds(pl.multiple_of((1 - core) * half, half), half)]
    count = near.shape[0]
    ways = count + far.shape[0]
    copies = []
    for i in range(0, ways, 4):
        ours, theirs, at = (near, other, i) if i < count else (far, far_other, i - count)
        wide = lambda blocks: jnp.concatenate([blocks[at + n] for n in range(4)], 1)
        both = jnp.dot(left, wide(ours), preferred_element_type=jnp.float32) + jnp.dot(
            right, wide(theirs), preferred_element_type=jnp.float32
        )
        for n in range(4):
            plane, dz = (1, 2, 0, 3)[(i + n) // (ways // 4)], (i + n) % (ways // 4)
            owner = lax.bitwise_xor(lax.rem(row + 4 * dz, ways), plane)
            columns = pl.ds(pl.multiple_of(owner * LANES, LANES), LANES)
            held[:, columns] = both[:, n * LANES : (n + 1) * LANES].astype(jnp.bfloat16)
            copies.append(pltpu.make_async_copy(held.at[:, columns], out.at[:, columns], sems.at[i + n]))
            copies[-1].start()
    for copy in copies:
        copy.wait()


def vmem(count):
    return [pl.BlockSpec(memory_space=pltpu.VMEM)] * count


def shards(tokens, proj_in, proj_out):
    return fast_shards(tokens, proj_in, proj_out)


def fast_shards(tokens, proj_in, proj_out):
    seq_rows = tokens[0]
    span, _ = seq_rows.shape
    depth, features = proj_in.shape
    ways = lax.axis_size("row")
    groups = features // GRP
    quarters = ways // groups
    pairs = GRP // 2 // quarters
    bf16, f32 = jnp.bfloat16, jnp.float32
    room = pltpu.CompilerParams(vmem_limit_bytes=16 << 20)

    me = lax.axis_index("col")
    half = features // 2
    swap_cores = lambda v: lax.ppermute(v, "col", [(0, 1), (1, 0)])
    along = lambda v, to: lax.ppermute(v, ("row", "col"), [(2 * r + c, 2 * to(r, c) + c) for r in range(ways) for c in (0, 1)])
    other_w = swap_cores(proj_in)
    table = jnp.asarray(channel_table(quarters, pairs), bf16)
    swap = np.zeros((GRP, GRP))
    swap[np.arange(GRP), channel_order(1, quarters, pairs)] = 1
    swap = jnp.asarray(swap, bf16)
    hbm = pl.BlockSpec(memory_space=pltpu.MemorySpace.HBM)
    smem = pl.BlockSpec(memory_space=pltpu.SMEM)
    mine = pl.pallas_call(
        fetch_kernel,
        in_specs=[smem] + [hbm] * 2,
        out_specs=vmem(1)[0],
        out_shape=jax.ShapeDtypeStruct((half, LANES), bf16),
        scratch_shapes=[
            pltpu.VMEM((half, LANES), bf16),
            pltpu.VMEM((GRP, GRP), bf16),
            pltpu.SemaphoreType.DMA((2,)),
        ],
        cost_estimate=pl.CostEstimate(flops=1 << 32, bytes_accessed=4 << 20, transcendentals=0),
        compiler_params=room,
        name="fetch",
    )(me[None], *[pltpu.with_memory_space_constraint(v, pltpu.MemorySpace.HBM) for v in (proj_out, swap)])
    ring = [mine]
    for dz in range(1, ways // 4):
        ring.append(along(mine, lambda r, c: (r - 4 * dz) % ways))
    sent = pl.pallas_call(
        send_kernel,
        in_specs=[smem] + vmem(4),
        out_specs=vmem(1)[0],
        out_shape=jax.ShapeDtypeStruct((ways, 48, LANES), bf16),
        scratch_shapes=[pltpu.VMEM((2 * LANES, features), bf16)],
        cost_estimate=pl.CostEstimate(flops=2 * span * depth * features, bytes_accessed=2 << 20, transcendentals=0),
        compiler_params=room,
        name="send",
    )(me[None], seq_rows, proj_in, other_w, table)
    *ring, _ = lax.optimization_barrier((*ring, sent))
    ring = jnp.stack(ring, 0)
    planes = []
    for flip in (1, 2, 3):
        planes.append(along(ring, lambda r, c: r ^ flip))
    held = lax.all_to_all(sent, "row", 0, 0, tiled=True)

    even, odd = position_tables(ways, span)
    even, odd = jnp.asarray(even, bf16), jnp.asarray(odd, bf16)
    twist = jnp.asarray(twiddle_table(ways, span), f32)
    special = lax.rem(lax.axis_index("row"), quarters)[None]
    spectra = pl.pallas_call(
        mix_kernel,
        in_specs=[pl.BlockSpec(memory_space=pltpu.SMEM)] + vmem(4),
        out_specs=vmem(1)[0],
        out_shape=jax.ShapeDtypeStruct((ways, 48, LANES), bf16),
        scratch_shapes=[pltpu.VMEM((ways * 32, 4 * LANES), bf16)],
        compiler_params=room,
        name="mix",
    )(special, held, even, odd, twist)

    back = lax.all_to_all(spectra, "row", 0, 0, tiled=True)
    *planes, _ = lax.optimization_barrier((*planes, spectra))
    near = jnp.concatenate(planes[:2], 0)
    far = jnp.concatenate([ring, planes[2]], 0)
    other = swap_cores(near)
    far_other = swap_cores(far)
    hot = jnp.asarray(row_order(span), bf16)
    place = jnp.stack([lax.axis_index("row"), me])
    wide = ways * LANES
    result = pl.pallas_call(
        out_kernel,
        in_specs=[smem] + vmem(6),
        out_specs=hbm,
        out_shape=jax.ShapeDtypeStruct((span, wide), bf16),
        scratch_shapes=[
            pltpu.VMEM((span, features), bf16),
            pltpu.VMEM((span, features), bf16),
            pltpu.VMEM((span, wide), bf16),
            pltpu.SemaphoreType.DMA((ways,)),
        ],
        cost_estimate=pl.CostEstimate(flops=2 * span * wide * features, bytes_accessed=4 << 20, transcendentals=0),
        compiler_params=room,
        name="out",
    )(place, back, hot, near, other, far, far_other)
    return result[None]


def fits(mesh, tokens, proj_in, proj_out):
    ways, cols = mesh.shape["row"], mesh.shape["col"]
    features = proj_in.shape[1]
    span = tokens.shape[1] // ways
    return (
        features % GRP == 0
        and ways == 4 * (features // GRP) == 16
        and span == 12 * ways
        and cols == 2
        and tokens.shape[0] == cols
        and proj_out.shape[1] == ways * LANES
    )


def solution(mesh):
    in_specs = (P("col", "row", None), P("col", None), P(None, "row"))
    out_specs = P("col", "row", None)

    def run(tokens, proj_in, proj_out):
        fast = fits(mesh, tokens, proj_in, proj_out)
        body = shards if fast else general_shards
        step = jax.shard_map(body, mesh=mesh, in_specs=in_specs, out_specs=out_specs, check_vma=False)
        return step(tokens, proj_in, proj_out)

    return run
```
